32 devices in a mesh: ep: 8 (over z, core), tp: 4 (over y, x).
Axes of the slice: x: 2, y: 2, z: 4, core: 2. Of those that a mesh axis runs over, the one named last changes fastest.
Arguments:
- conv_input: bfloat16 [1024, 16384], P('tp', 'ep'), may hold values from -6 to 6
- out_gate: bfloat16 [1024, 16384], P('tp', 'ep'), may hold values from -6 to 6
- in_gate: bfloat16 [1024, 16384], P('tp', 'ep'), may hold values from -6 to 6
- conv_taps: float32 [3, 1024], replicated, may hold values from -3.5 to 3.5
- mixer_proj: bfloat16 [1024, 2048], P(None, 'tp'), may hold values from -0.1875 to 0.1875
- token_rows: bfloat16 [2048, 2048], P('ep', 'tp'), may hold values from -4000 to 4000
- routes: int32 [2048, 2], P('ep'), may hold values from 0 to 7, as said below
- route_weights: float32 [2048, 2], P('ep'), may hold values from 0.3 to 1
- expert_gate: bfloat16 [8, 2048, 4096], P('ep', None, 'tp'), may hold values from -0.125 to 0.125
- expert_up: bfloat16 [8, 2048, 4096], P('ep', None, 'tp'), may hold values from -0.125 to 0.125
- expert_down: bfloat16 [8, 4096, 2048], P('ep', 'tp'), may hold values from -0.125 to 0.125
Outputs:
- mixed_out: bfloat16 [16384, 2048], P('ep', 'tp')
- expert_out: bfloat16 [2048, 2048], P('ep', 'tp')
The draws below stay inside these ranges and needn't reach their ends.
Inputs may be any that keep to these rules, and one draw needn't show every extreme that they name: `routes`: in each aligned block of 256 rows, no expert is named more than 128 times and one expert, the same in every block, exactly 128 times; the two experts of a row differ.
All inputs are finite; a program needn't handle non-finite values.
Results may differ from the reference program's by a relative error of at most 0.015.
Values may be sent and summed in bfloat16 or wider, within the bound.
A program may use at most 64 MiB of HBM per device.

```python
import math
import jax
import jax.numpy as jnp
from jax import lax

D = 2048
W = 1024
FF = 4096
KERNEL = 3
ROWS_B = 256
EXPERTS = 8
FF_PART = 1024
TOK_A = 16384
TOK_B = 2048
CAP = 128
N_TP = 4


def draw_token_rows(key, part):
    base_key, row_key, col_key = jax.random.split(key, 3)
    ramp = jnp.arange(D, dtype=jnp.float32) / D
    base = jnp.clip(jax.random.normal(base_key, (TOK_B, D), jnp.float32), -6.0, 6.0)
    row_scales = jnp.exp(jax.random.uniform(row_key, (TOK_B, 1), jnp.float32, 0.0, math.log(10.0)))
    col_scales = jnp.exp(math.log(10.0) * ramp) * jnp.exp(jax.random.uniform(col_key, (D,), jnp.float32, -0.4, 0.4))
    return (base * row_scales * col_scales[None, :]).astype(jnp.bfloat16)


def draw_routes(key, part):
    blocks = TOK_B // ROWS_B
    capacity = 4 * ROWS_B // EXPERTS
    spare = 2 * ROWS_B - capacity
    hottest = jax.random.randint(jax.random.fold_in(key, 7), (), 0, EXPERTS).astype(jnp.int32)
    ladder = jnp.arange(EXPERTS - 1, dtype=jnp.int32)
    weight_cum = (ladder + 1) * (ladder + 2) // 2
    weight_total = (EXPERTS - 1) * EXPERTS // 2
    run_ends = capacity + spare * weight_cum // weight_total
    position = jnp.arange(2 * ROWS_B, dtype=jnp.int32)
    which_run = jnp.sum((position[:, None] >= run_ends[None, :]).astype(jnp.int32), axis=1)
    which_run = jnp.minimum(which_run, EXPERTS - 2)

    def one_block(block_index):
        block_key = jax.random.fold_in(key, block_index + 11)
        order = jax.random.permutation(jax.random.fold_in(block_key, 1), EXPERTS - 1).astype(jnp.int32)
        others = (hottest + 1 + order) % EXPERTS
        listing = jnp.where(position < capacity, hottest, others[which_run])
        pairs = jnp.stack([listing[:ROWS_B], listing[ROWS_B:]], axis=1)
        shuffle = jax.random.permutation(jax.random.fold_in(block_key, 2), ROWS_B)
        return pairs[shuffle]
    table = jax.vmap(one_block)(jnp.arange(blocks, dtype=jnp.int32))
    return table.reshape(TOK_B, 2).astype(jnp.int32)


def spiked(drawn, rng, source, target, shards_of, factor):
    owner, partner = [(jnp.arange(drawn.shape[axis_at]) // (drawn.shape[axis_at] // shards_of)).reshape([-1 if axis == axis_at else 1 for axis in range(drawn.ndim)]) for axis_at in (source, target)]
    chosen = jax.random.permutation(rng, shards_of)[partner]
    strong = (owner == chosen) | (owner == (partner + shards_of // 2) % shards_of)
    return jnp.where(strong, factor * drawn, drawn)


def levels(rng, dims, shards, least, largest):
    def one(dim, blocks):
        heights = jax.random.uniform(jax.random.fold_in(jax.random.fold_in(rng, 6), dim), (blocks,), jnp.float32, least / len(shards), largest / len(shards))
        return jnp.repeat(jnp.exp(heights), dims[dim] // blocks).reshape((-1,) + (1,) * (len(dims) - dim - 1))

    factor_of = one(*shards[0])
    for cut in shards[1:]:
        factor_of = factor_of * one(*cut)
    return factor_of


def bell_draw(key, extent, scale, limit, pieces=(), kind=jnp.bfloat16):
    result = jax.random.normal(key, extent, jnp.float32) * scale
    if len(pieces) > 0:
        result = levels(key, extent, pieces, -0.22, 0.18) * result
    return jnp.clip(result, min=-limit, max=limit).astype(kind)


def noise_with(rng, shape, width, bound, cuts, heavy, held_as=jnp.bfloat16):
    drawn = width * jax.random.normal(rng, shape, jnp.float32)
    if cuts:
        drawn = drawn * levels(rng, shape, cuts, -0.22, 0.18)
    return jnp.clip(spiked(drawn, jax.random.fold_in(rng, 3), *heavy), -bound, bound).astype(held_as)


def setup_inputs(seed: int = 0) -> dict:
    seeds = jax.random.split(jax.random.key(seed), 12)
    return {
        "conv_input": bell_draw(seeds[0], (W, TOK_A), 1.0, 6.0, ((0, 4), (1, 8))),
        "out_gate": bell_draw(seeds[1], (W, TOK_A), 1.0, 6.0, ((0, 4), (1, 8))),
        "in_gate": bell_draw(seeds[2], (W, TOK_A), 1.0, 6.0, ((0, 4), (1, 8))),
        "conv_taps": bell_draw(seeds[3], (KERNEL, W), 0.6, 3.5, (), jnp.float32),
        "mixer_proj": bell_draw(seeds[4], (W, D), W ** -0.5, 0.1875, ((1, 4),)),
        "token_rows": draw_token_rows(jax.random.fold_in(seeds[11], 71), 0),
        "routes": draw_routes(jax.random.fold_in(seeds[11], 71), 0),
        "route_weights": jnp.clip(0.3 + 0.7 * jax.random.uniform(seeds[7], (TOK_B, 2), jnp.float32) ** levels(seeds[7], (TOK_B, 2), ((0, 8),), -0.2, 0.2), 0.3, 1.0),
        "expert_gate": bell_draw(seeds[8], (EXPERTS, D, FF), D ** -0.5, 0.125, ((0, 8), (2, 4))),
        "expert_up": bell_draw(seeds[9], (EXPERTS, D, FF), D ** -0.5, 0.125, ((0, 8), (2, 4))),
        "expert_down": noise_with(seeds[10], (EXPERTS, FF, D), FF ** -0.5, 0.125, ((0, 8), (1, 4)), (1, 2, 4, 2.0)),
    }


EPSILON = 1e-06

def slot_places(route_ids, capacity, experts):
    flat_ids = route_ids.reshape(-1).astype(jnp.int32)
    hit_table = (flat_ids[:, None] == jnp.arange(experts, dtype=jnp.int32)[None, :]).astype(jnp.int32)
    earlier = jnp.cumsum(hit_table, axis=0) - hit_table
    slot_rank = lax.optimization_barrier(jnp.sum(earlier * hit_table, axis=1))
    return (flat_ids * capacity + slot_rank).astype(jnp.int32)

def mixer(conv_input, out_gate, in_gate, conv_taps, mixer_proj):
    z_rows = (conv_input.astype(jnp.float32) * in_gate.astype(jnp.float32)).astype(jnp.bfloat16)
    length = z_rows.shape[1]
    padded = jnp.pad(z_rows.astype(jnp.float32), ((0, 0), (KERNEL - 1, 0)))
    conv_sum = jnp.zeros(z_rows.shape, jnp.float32)
    for lag_index in range(KERNEL):
        begin = KERNEL - 1 - lag_index
        conv_sum = conv_sum + conv_taps[lag_index][:, None] * padded[:, begin:begin + length]
    gated = (out_gate.astype(jnp.float32) * conv_sum).astype(jnp.bfloat16)
    return jnp.dot(gated.T, mixer_proj, preferred_element_type=jnp.float32).astype(jnp.bfloat16)

def expert_block(inputs):
    rows_in, gate_weight, up_weight, down_weight = inputs
    values = rows_in.astype(jnp.float32)
    row_scale = lax.rsqrt(lax.optimization_barrier(jnp.mean(values * values, axis=1, keepdims=True)) + EPSILON)
    gate_sum = row_scale * jnp.dot(rows_in, gate_weight, preferred_element_type=jnp.float32)
    up_sum = row_scale * jnp.dot(rows_in, up_weight, preferred_element_type=jnp.float32)
    hidden = (jax.nn.silu(gate_sum) * up_sum).astype(jnp.bfloat16)
    split_hidden = hidden.reshape(hidden.shape[0], N_TP, FF_PART).astype(jnp.float32)
    split_down = down_weight.reshape(N_TP, FF_PART, D).astype(jnp.float32)
    partial_value = jnp.einsum('snf,nfd->nsd', split_hidden, split_down).astype(jnp.bfloat16)
    return lax.optimization_barrier(jnp.sum(partial_value.astype(jnp.float32), axis=0)).astype(jnp.bfloat16)

def reference(conv_input, out_gate, in_gate, conv_taps, mixer_proj, token_rows, routes, route_weights, expert_gate, expert_up, expert_down):
    mixed_out = mixer(conv_input, out_gate, in_gate, conv_taps, mixer_proj)
    blocks = TOK_B // ROWS_B
    route_blocks = routes.reshape(blocks, ROWS_B, 2)

    def block_places(route_ids):
        return slot_places(route_ids, CAP, EXPERTS)
    places = jax.vmap(block_places)(route_blocks)
    sources = jnp.arange(2 * ROWS_B, dtype=jnp.int32) // 2

    def fill(rows_in, place_list):
        return jnp.zeros((EXPERTS * CAP, D), jnp.bfloat16).at[place_list].set(rows_in[sources])
    buffers = jax.vmap(fill)(token_rows.reshape(blocks, ROWS_B, D), places)
    by_expert = buffers.reshape(blocks, EXPERTS, CAP, D).transpose(1, 0, 2, 3).reshape(EXPERTS, blocks * CAP, D)
    results = lax.map(expert_block, (by_expert, expert_gate, expert_up, expert_down))
    home = results.reshape(EXPERTS, blocks, CAP, D).transpose(1, 0, 2, 3).reshape(blocks, EXPERTS * CAP, D)

    def pick(rows_in, place_list):
        return rows_in[place_list]
    picked = jax.vmap(pick)(home, places).astype(jnp.float32).reshape(blocks, ROWS_B, 2, D)
    weights = route_weights.reshape(blocks, ROWS_B, 2, 1)
    expert_out = lax.optimization_barrier(jnp.sum(picked * weights, axis=2)).reshape(TOK_B, D).astype(jnp.bfloat16)
    return (mixed_out, expert_out)
```

```python
import functools

import jax
import jax.numpy as jnp
from jax import lax
from jax.experimental import pallas as pl
from jax.experimental.pallas import tpu as pltpu
from jax.sharding import PartitionSpec as P

KERNEL = 3
EPSILON = 1e-06
LANES = 128
CHUNKS = 8
PIECES = 2
MESH = pl.DeviceIdType.MESH


def pick(index, values):
    out = jnp.int32(values[-1])
    for i in range(len(values) - 1):
        out = jnp.where(index == i, jnp.int32(values[i]), out)
    return out


def aligned(start, size):
    return pl.ds(pl.multiple_of(start, size), size)


def fused_kernel(
    early_rows,
    conv_input, out_gate, in_gate, taps, proj_in, tokens, routes, weights, gate_in, up_in, down_in,
    mixed_out, expert_out,
    x, wg, wu, wd, cin, cig, cog, zb, y, proj, tap_buf, tap_in, route_buf, weight_buf,
    tabs, wcols, hidden, part_out, part_in, sums, one, two_out, two_in, tot, tot_in, mixed, final,
    load_sem, s_xy, r_xy, s_z, r_z, s_pc, r_pc, s_tab, r_tab, s_rim, r_rim, s_mix, r_mix,
    s_part, r_part, s_one, r_one, s_two, r_two, s_tot, r_tot, out_sem,
):
    rows, part = tokens.shape
    blocks = x.shape[0] // rows
    levels = blocks // 2
    features = x.shape[1]
    units = wg.shape[1]
    width, length = conv_input.shape
    step = length // CHUNKS
    half = rows // 2
    ep, here = lax.axis_index("ep"), lax.axis_index("tp")
    level, core = ep // 2, ep % 2
    end = (level == 0) | (level == levels - 1)

    def device(level_to, core_to, tp_to):
        return {"ep": level_to * 2 + core_to, "tp": tp_to}

    xn, yn = device(level, core, here ^ 1), device(level, core, here ^ 2)
    pc = device(level, 1 - core, here)

    def remote(src, dst, send_sem, recv_sem, target):
        return pltpu.make_async_remote_copy(
            src_ref=src, dst_ref=dst, send_sem=send_sem, recv_sem=recv_sem,
            device_id=target, device_id_type=MESH,
        )

    def each(begin, stop, action):
        def run(i, carry):
            action(i)
            return carry

        lax.fori_loop(begin, stop, run, 0)

    def order(k):
        return jnp.where(
            k == 0, level,
            pick(level * 4 + k, [0, 1, 2, 3, 1, 2, 0, 3, 2, 1, 3, 0, 3, 2, 1, 0]),
        )

    barrier = pltpu.get_barrier_semaphore()
    for target in [xn, yn, pc]:
        pl.semaphore_signal(barrier, inc=1, device_id=target, device_id_type=MESH)
    for away in range(1, levels):
        pl.semaphore_signal(
            barrier, inc=1, device_id=device((level + away) % levels, core, here),
            device_id_type=MESH,
        )
    has_next, has_prev = ep < blocks - 1, ep > 0
    far_rim = ((core == 1) & has_next) | ((core == 0) & has_prev)
    rim_ep = jnp.where(core == 1, ep + 1, ep - 1)

    @pl.when(far_rim)
    def _():
        pl.semaphore_signal(
            barrier, inc=1, device_id={"ep": rim_ep, "tp": here}, device_id_type=MESH
        )

    def block_rows(level_of, core_of, begin=0, size=None):
        size = rows if size is None else size
        return pl.ds(pl.multiple_of((level_of * 2 + core_of) * rows + begin, 16), size)

    def cols(relative):
        return aligned((here ^ relative) * part, part)

    own_at = x.at[block_rows(level, core), cols(0)]
    loads = [
        (routes, route_buf), (weights, weight_buf), (taps, tap_in), (tokens, own_at),
        (conv_input, cin), (in_gate, cig), (out_gate, cog), (gate_in, wg), (up_in, wu),
        (down_in, wd), (proj_in, proj),
    ]
    loads = [
        pltpu.make_async_copy(src, dst, load_sem.at[i]) for i, (src, dst) in enumerate(loads)
    ]
    for copy in loads:
        copy.start()

    names = lax.broadcasted_iota(jnp.int32, (blocks, rows), 0)
    for copy in loads[:3]:
        copy.wait()
    table = jnp.zeros((blocks, rows), jnp.float32)
    for k in range(2):
        table = table + jnp.where(route_buf[k : k + 1, :] == names, weight_buf[k : k + 1, :], 0.0)
    tabs[ep] = table
    tap_buf[...] = jnp.zeros_like(tap_buf)
    tap_buf[0:KERNEL, :] = tap_in[:, aligned(here * width, width)]
    tap_cols = jnp.transpose(tap_buf[...])
    wcols[...] = jnp.zeros_like(wcols)

    for copy in loads[4:6]:
        copy.wait()

    def make_z(q):
        at = aligned(q * step, step)
        value = cin[:, at].astype(jnp.float32) * cig[:, at].astype(jnp.float32)
        zb[:, pl.ds(pl.multiple_of(q * step + LANES, LANES), step)] = value.astype(jnp.bfloat16)

    make_z(CHUNKS - 1)
    loads[3].wait()
    pl.semaphore_wait(barrier, 2 + levels + far_rim.astype(jnp.int32))

    def plane(level_of, way, low):
        size = rows - low
        lower = (size // 2 + 15) // 16 * 16
        begin, count, relative, target = (
            (low, size, 0, xn), (low, size, 0, yn),
            (low, lower, 1, yn), (low + lower, size - lower, 2, xn),
        )[way]
        at = x.at[block_rows(level_of, core, begin, count), cols(relative)]
        sem = level_of * 4 + way
        return remote(at, at, s_xy.at[sem], r_xy.at[sem], target)

    def along(level_of, relative, up):
        at = x.at[
            block_rows(level_of, core, 0, rows if relative == 0 else early_rows), cols(relative)
        ]
        side = level_of * 8 + relative * 2 + jnp.where(up, 1, 0)
        target = device(jnp.where(up, level + 1, level - 1), core, here)
        return remote(at, at, s_z.at[side], r_z.at[level_of * 4 + relative], target)

    def partner(level_of, relative):
        at = x.at[block_rows(level_of, core), cols(relative)]
        sem = level_of * 4 + relative
        return remote(at, at, s_pc.at[sem], r_pc.at[sem], pc)

    def spread(relative):
        @pl.when(level < levels - 1)
        def _():
            along(level, relative, True).start()

        @pl.when(level > 0)
        def _():
            along(level, relative, False).start()

    def table_to(away):
        target = device((level + away) % levels, core, here)
        return remote(tabs.at[ep], tabs.at[ep], s_tab.at[away], r_tab.at[ep], target)

    def table_pc(level_of):
        at = tabs.at[level_of * 2 + core]
        return remote(at, at, s_tab.at[levels + level_of], r_tab.at[level_of * 2 + core], pc)

    def table_wait(block):
        at = tabs.at[block]
        remote(at, at, s_tab.at[0], r_tab.at[block], pc).wait_recv()

    rim_copy = remote(
        zb.at[:, pl.ds(length, LANES)], zb.at[:, pl.ds(0, LANES)], s_rim, r_rim,
        {"ep": jnp.where(has_next, ep + 1, ep), "tp": here},
    )

    spread(0)
    plane(level, 0, 0).start()
    plane(level, 1, 0).start()
    partner(level, 0).start()

    @pl.when(has_next)
    def _():
        rim_copy.start()

    for away in range(1, levels):
        table_to(away).start()
    table_pc(level).start()

    each(0, CHUNKS - 1, make_z)
    loads[6].wait()

    own_channels = aligned(here * width, width)

    def conv_chunk(q):
        at = aligned(q * step, step)
        value = zb[:, pl.ds(pl.multiple_of(q * step, LANES), step + LANES)].astype(jnp.float32)
        total = jnp.zeros((width, step), jnp.float32)
        for lag in range(KERNEL):
            moved = pltpu.roll(value, lag, 1) if lag else value
            total = total + tap_cols[:, lag : lag + 1] * moved[:, LANES:]
        y[own_channels, at] = (cog[:, at].astype(jnp.float32) * total).astype(jnp.bfloat16)

    each(1, CHUNKS, conv_chunk)

    @pl.when(has_prev)
    def _():
        rim_copy.wait_recv()

    @pl.when(jnp.logical_not(has_prev))
    def _():
        zb[:, 0:LANES] = jnp.zeros((width, LANES), jnp.bfloat16)

    conv_chunk(0)

    def mix(q, way):
        at = aligned(q * step, step)
        if way < 2:
            src, target = y.at[own_channels, at], (xn, yn)[way]
            sem = q * 3 + way
        else:
            src = y.at[aligned((here ^ way // 2) * width, width), at]
            target = {2: yn, 4: xn}[way]
            sem = q * 3 + 2
        return remote(src, src, s_mix.at[sem], r_mix.at[sem], target)

    def mix_event(n):
        @pl.when(n < CHUNKS)
        def _():
            mix(n, 0).start()
            mix(n, 1).start()

        @pl.when(n >= CHUNKS)
        def _():
            q = n - CHUNKS

            @pl.when(q % 2 == 0)
            def _():
                mix(q, 0).wait_recv()
                mix(q, 2).start()

            @pl.when(q % 2 == 1)
            def _():
                mix(q, 1).wait_recv()
                mix(q, 4).start()

    each(0, 2, mix_event)

    plane(level, 0, 0).wait_recv()
    plane(level, 2, 0).start()
    spread(1)
    partner(level, 1).start()
    plane(level, 1, 0).wait_recv()
    plane(level, 3, 0).start()
    spread(2)
    partner(level, 2).start()
    for away in range(1, levels):
        other = (level + away) % levels
        table_wait(other * 2 + core)
        table_pc(other).start()
    each(2, 4, mix_event)
    plane(level, 2, 0).wait_recv()
    plane(level, 3, 0).wait_recv()
    spread(3)
    partner(level, 3).start()

    def comm_first(k):
        from_level = order(k)
        up = from_level < level
        relay = jnp.where(up, level < levels - 1, level > 0)
        for relative in range(4):
            along(from_level, relative, up).wait_recv()

            @pl.when(relay)
            def _():
                along(from_level, relative, up).start()

            if relative == 0:
                plane(from_level, 0, early_rows).start()
                plane(from_level, 1, early_rows).start()
                partner(from_level, 0).start()

    def comm_second(k):
        from_level = order(k)
        plane(from_level, 0, early_rows).wait_recv()
        plane(from_level, 2, early_rows).start()
        partner(from_level, 1).start()
        plane(from_level, 1, early_rows).wait_recv()
        plane(from_level, 3, early_rows).start()
        partner(from_level, 2).start()
        plane(from_level, 2, early_rows).wait_recv()
        plane(from_level, 3, early_rows).wait_recv()
        partner(from_level, 3).start()

    def one_copy(k, relative, axis):
        begin = 0 if axis == 0 else half
        at = sums.at[k, relative, pl.ds(begin, half)]
        slot = {(1, 0): 0, (3, 0): 1, (2, 1): 0, (3, 1): 1}[relative, axis]
        sem = (k * 2 + axis) * 2 + slot
        return remote(at, one.at[k, axis, slot], s_one.at[sem], r_one.at[sem], (xn, yn)[axis])

    def two_copy(k, axis):
        sem = k * 2 + axis
        return remote(
            two_out.at[k, axis], two_in.at[k, axis], s_two.at[sem], r_two.at[sem], (yn, xn)[axis]
        )

    def total_copy(k):
        to = order(k)
        return remote(
            tot.at[k], tot_in.at[level], s_tot.at[k], r_tot.at[level], device(to, core, here)
        )

    def part_copy(k, relative):
        sem = k * 4 + relative
        return remote(
            part_out.at[k, relative], part_in.at[k, relative], s_part.at[sem], r_part.at[sem], pc
        )

    def second_stage(k):
        for axis, relative in ((0, 2), (1, 1)):
            begin = 0 if axis == 0 else half
            one_copy(k, (1, 2)[axis], axis).wait_recv()
            one_copy(k, 3, axis).wait_recv()
            two_out[k, axis] = (
                sums[k, relative, begin : begin + half].astype(jnp.float32)
                + one[k, axis, 1].astype(jnp.float32)
            ).astype(jnp.bfloat16)
            two_copy(k, axis).start()

    def third_stage(k):
        to = order(k)
        for axis in range(2):
            begin = 0 if axis == 0 else half
            two_copy(k, axis).wait_recv()
            tot[k, begin : begin + half] = (
                sums[k, 0, begin : begin + half].astype(jnp.float32)
                + one[k, axis, 0].astype(jnp.float32)
                + two_in[k, axis].astype(jnp.float32)
            ).astype(jnp.bfloat16)

        @pl.when(to != level)
        def _():
            total_copy(k).start()

        @pl.when(to == level)
        def _():
            tot_in[level] = tot[k]

    def column_of(block):
        lane = lax.broadcasted_iota(jnp.int32, (rows, LANES), 1)
        return jnp.sum(jnp.where(lane == block, wcols[...], 0.0), axis=1, keepdims=True)

    tile = min(256, units)

    def iteration(k):
        from_level = order(k)

        each(
            jnp.where(end, pick(k, [1, 2, 2, 3]), pick(k, [1, 3, 4, 4])),
            jnp.where(end, pick(k, [2, 2, 3, 4]), pick(k, [3, 3, 4, 4])),
            comm_first,
        )

        @pl.when(k > 0)
        def _():
            comm_second(k)

        each(
            jnp.where(end, 4, pick(k, [4, 3, 4, 4])),
            4,
            comm_first,
        )
        each(pick(k, [4, 8, 12, 14]), pick(k, [8, 12, 14, 16]), mix_event)
        for relative in range(4):
            at = x.at[block_rows(from_level, 1 - core), cols(relative)]
            remote(
                at, at, s_pc.at[0], r_pc.at[from_level * 4 + relative], pc
            ).wait_recv()

        pair = pl.ds(pl.multiple_of(from_level * 2 * rows, 2 * rows), 2 * rows)
        squares = jnp.zeros((2 * rows, LANES), jnp.float32)
        for first in range(0, features, LANES):
            value = x[pair, first : first + LANES].astype(jnp.float32)
            squares = squares + value * value
        scale = lax.rsqrt(jnp.sum(squares, axis=1, keepdims=True) / features + EPSILON)

        def hidden_tile(n):
            at = aligned(n * tile, tile)
            rows_in = x[pair, :]
            gate = scale * jnp.dot(rows_in, wg[:, at], preferred_element_type=jnp.float32)
            up = scale * jnp.dot(rows_in, wu[:, at], preferred_element_type=jnp.float32)
            hidden[:, at] = (gate / (1.0 + jnp.exp(-gate)) * up).astype(jnp.bfloat16)

        each(0, units // tile, hidden_tile)

        @pl.when(k > 0)
        def _():
            second_stage(k - 1)

        def product(core_of, relative):
            value = hidden[aligned(core_of * rows, rows), :]
            weight = wd[:, cols(relative)]
            return column_of(from_level * 2 + core_of) * jnp.dot(
                value, weight, preferred_element_type=jnp.float32
            )

        for relative in (3, 1, 2, 0):
            part_out[k, relative] = product(1 - core, relative).astype(jnp.bfloat16)
            part_copy(k, relative).start()
        for relative in (3, 1, 2, 0):
            value = product(core, relative)
            part_copy(k, relative).wait_recv()
            sums[k, relative] = (value + part_in[k, relative].astype(jnp.float32)).astype(
                jnp.bfloat16
            )
            for axis in range(2):
                if relative in (3, axis + 1):
                    one_copy(k, relative, axis).start()

        @pl.when(k > 0)
        def _():
            third_stage(k - 1)

    for away in range(levels):
        table_wait((level + away) % levels * 2 + 1 - core)
    for block in range(blocks):
        wcols_at = tabs[block, pl.ds(ep, 1), :]
        tap_buf[block : block + 1, :] = wcols_at
    wcols[...] = jnp.transpose(tap_buf[...])
    for copy in loads[7:]:
        copy.wait()

    each(0, levels, iteration)

    def mix_tile(q):
        @pl.when(q % 2 == 0)
        def _():
            mix(q, 1).wait_recv()

        @pl.when(q % 2 == 1)
        def _():
            mix(q, 0).wait_recv()

        mix(q, 2).wait_recv()
        at = aligned(q * step, step)
        mixed[at, :] = lax.dot_general(
            y[:, at], proj[...], (((0,), (0,)), ((), ())), preferred_element_type=jnp.float32
        ).astype(jnp.bfloat16)
        pltpu.make_async_copy(mixed.at[at], mixed_out.at[at], out_sem.at[q]).start()

    each(0, CHUNKS, mix_tile)
    second_stage(levels - 1)
    third_stage(levels - 1)
    for away in range(1, levels):
        source = (level + away) % levels
        at = tot_in.at[source]
        remote(at, at, s_tot.at[0], r_tot.at[source], xn).wait_recv()
    answer = jnp.zeros((rows, part), jnp.float32)
    for source in range(levels):
        answer = answer + tot_in[source].astype(jnp.float32)
    final[...] = answer.astype(jnp.bfloat16)
    last = pltpu.make_async_copy(final, expert_out, out_sem.at[CHUNKS])
    last.start()

    for relative in range(4):
        @pl.when(level < levels - 1)
        def _():
            along(level, relative, True).wait_send()

        @pl.when(level > 0)
        def _():
            along(level, relative, False).wait_send()

        partner(level, relative).wait_send()
        plane(level, relative, 0).wait_send()

    @pl.when(has_next)
    def _():
        rim_copy.wait_send()

    for away in range(1, levels):
        table_to(away).wait_send()
    for level_of in range(levels):
        table_pc(level_of).wait_send()

    def finish(k):
        from_level = order(k)
        up = from_level < level
        relay = jnp.where(up, level < levels - 1, level > 0)
        for relative in range(4):
            @pl.when((k > 0) & relay)
            def _():
                along(from_level, relative, up).wait_send()

            @pl.when(k > 0)
            def _():
                plane(from_level, relative, early_rows).wait_send()
                partner(from_level, relative).wait_send()

            part_copy(k, relative).wait_send()
        for axis in range(2):
            one_copy(k, axis + 1, axis).wait_send()
            one_copy(k, 3, axis).wait_send()
            two_copy(k, axis).wait_send()

        @pl.when(from_level != level)
        def _():
            total_copy(k).wait_send()

    each(0, levels, finish)

    def finish_mix(q):
        for way in range(3):
            mix(q, way).wait_send()
        at = aligned(q * step, step)
        pltpu.make_async_copy(mixed.at[at], mixed_out.at[at], out_sem.at[q]).wait()

    each(0, CHUNKS, finish_mix)
    last.wait()


def fused(*args):
    (conv_input, out_gate, in_gate, conv_taps, mixer_proj, token_rows, routes, route_weights,
     expert_gate, expert_up, expert_down) = args
    tp, experts = lax.axis_size("tp"), lax.axis_size("ep")
    rows, part = token_rows.shape
    features = part * tp
    units = expert_gate.shape[2]
    width, length = conv_input.shape
    levels, half = experts // 2, rows // 2
    early_rows = rows * 5 // 8 // 16 * 16
    bf16, f32 = jnp.bfloat16, jnp.float32
    dma = pltpu.SemaphoreType.DMA
    hold = pltpu.VMEM
    scratch = [
        hold((experts * rows, features), bf16),
        hold((features, units), bf16), hold((features, units), bf16), hold((units, features), bf16),
        hold((width, length), bf16), hold((width, length), bf16), hold((width, length), bf16),
        hold((width, length + LANES), bf16),
        hold((tp * width, length), bf16),
        hold(mixer_proj.shape, bf16),
        hold((LANES, max(width, rows)), f32),
        hold(conv_taps.shape, f32),
        hold((2, rows), jnp.int32), hold((2, rows), f32),
        hold((experts, experts, rows), f32),
        hold((rows, LANES), f32),
        hold((2 * rows, units), bf16),
        hold((levels, 4, rows, part), bf16), hold((levels, 4, rows, part), bf16),
        hold((levels, 4, rows, part), bf16),
        hold((levels, 2, 2, half, part), bf16),
        hold((levels, 2, half, part), bf16), hold((levels, 2, half, part), bf16),
        hold((levels, rows, part), bf16), hold((levels, rows, part), bf16),
        hold((length, part), bf16),
        hold((rows, part), bf16),
        dma((11,)),
        dma((levels * 4,)), dma((levels * 4,)),
        dma((levels * 8,)), dma((levels * 4,)),
        dma((levels * 4,)), dma((levels * 4,)),
        dma((levels * 2,)), dma((experts,)),
        dma, dma,
        dma((CHUNKS * 3,)), dma((CHUNKS * 3,)),
        dma((levels * 4,)), dma((levels * 4,)),
        dma((levels * 4,)), dma((levels * 4,)),
        dma((levels * 2,)), dma((levels * 2,)),
        dma((levels,)), dma((levels,)),
        dma((CHUNKS + 1,)),
    ]
    anywhere = pl.BlockSpec(memory_space=pl.ANY)
    return pl.pallas_call(
        functools.partial(fused_kernel, early_rows),
        out_shape=(
            jax.ShapeDtypeStruct((length, part), bf16), jax.ShapeDtypeStruct((rows, part), bf16)
        ),
        in_specs=[anywhere] * 11,
        out_specs=(anywhere, anywhere),
        scratch_shapes=scratch,
        compiler_params=pltpu.CompilerParams(
            collective_id=0, has_side_effects=True, vmem_limit_bytes=67043328
        ),
    )(
        conv_input, out_gate, in_gate, conv_taps, mixer_proj, token_rows, routes.T,
        route_weights.T, expert_gate[0], expert_up[0], expert_down[0],
    )


def passed_along(value, axis, by):
    devices = lax.axis_size(axis)
    pairs = [(i, i + by) for i in range(devices) if 0 <= i + by < devices]
    return lax.ppermute(value, axis, pairs)


def rotated(value, by):
    devices = lax.axis_size("ep")
    return lax.ppermute(value, "ep", [(i, (i + by) % devices) for i in range(devices)])


def routing(route_ids, capacity, experts):
    rows = route_ids.shape[0]
    names = jnp.arange(experts, dtype=jnp.int32)[None, :]
    hits = [(route_ids[:, k][:, None] == names) for k in range(2)]
    both = (hits[0] | hits[1]).astype(jnp.bfloat16)
    index = jnp.arange(rows, dtype=jnp.int32)
    lower = (index[:, None] > index[None, :]).astype(jnp.bfloat16)
    earlier = jnp.dot(lower, both, preferred_element_type=jnp.float32)
    away = lax.rem(route_ids - lax.axis_index("ep") + experts, experts)
    places = []
    for k in range(2):
        rank = jnp.sum(jnp.where(hits[k], earlier, 0.0), axis=1).astype(jnp.int32)
        places.append(away[:, k] * capacity + rank)
    return places


def expert_hidden(part_in, row_scale, gate_weight, up_weight):
    gate_sum = jnp.dot(part_in, gate_weight, preferred_element_type=jnp.float32)
    up_sum = jnp.dot(part_in, up_weight, preferred_element_type=jnp.float32)
    return (jax.nn.silu(row_scale * gate_sum) * (row_scale * up_sum)).astype(jnp.bfloat16)


def product(hidden, down):
    return jnp.dot(hidden, down, preferred_element_type=jnp.float32).astype(jnp.bfloat16)


def general(
    conv_input,
    out_gate,
    in_gate,
    conv_taps,
    mixer_proj,
    token_rows,
    routes,
    route_weights,
    expert_gate,
    expert_up,
    expert_down,
):
    tp = lax.axis_size("tp")
    here = lax.axis_index("tp")
    width_part = conv_input.shape[0]
    length = conv_input.shape[1]
    local_taps = lax.dynamic_slice_in_dim(conv_taps, here * width_part, width_part, 1)

    experts = lax.axis_size("ep")
    rows_b, cols_part = token_rows.shape
    capacity = 4 * rows_b // experts
    slot_total = experts * capacity
    feature_count = cols_part * tp
    places = routing(routes, capacity, experts)
    slots = jnp.arange(slot_total, dtype=jnp.int32)
    picks = [(slots[:, None] == places[k][None, :]) for k in range(2)]
    chosen = (picks[0] | picks[1]).astype(jnp.bfloat16)
    buffer = jnp.dot(chosen, token_rows, preferred_element_type=jnp.float32).astype(jnp.bfloat16)

    z_rows = (conv_input.astype(jnp.float32) * in_gate.astype(jnp.float32)).astype(jnp.bfloat16)
    rim_rows = passed_along(z_rows[:, length - (KERNEL - 1) :], "ep", 1)
    longer = jnp.concatenate([rim_rows, z_rows], axis=1).astype(jnp.float32)
    conv_sum = jnp.zeros(z_rows.shape, jnp.float32)
    for lag_index in range(KERNEL):
        begin = KERNEL - 1 - lag_index
        conv_sum = conv_sum + local_taps[lag_index][:, None] * longer[:, begin : begin + length]
    gated = (out_gate.astype(jnp.float32) * conv_sum).astype(jnp.bfloat16)

    gated, buffer = lax.optimization_barrier((gated, buffer))
    arrived = [
        rotated(buffer[d * capacity : (d + 1) * capacity], d) if d else buffer[:capacity]
        for d in range(experts)
    ]
    chunk_parts = experts // PIECES
    chunks = [
        jnp.concatenate(arrived[c * chunk_parts : (c + 1) * chunk_parts], axis=0)
        for c in range(PIECES)
    ]
    gate_weight, up_weight, down_weight = expert_gate[0], expert_up[0], expert_down[0]

    def squares_of(part_in):
        return jnp.sum(jnp.square(part_in.astype(jnp.float32)), axis=1)

    def scale_of(squares):
        return lax.rsqrt(squares / feature_count + EPSILON)[:, None]

    outs, returned = [], []

    def send_back(c):
        for i in range(chunk_parts):
            d = c * chunk_parts + i
            block = outs[c][i * capacity : (i + 1) * capacity]
            returned.append(rotated(block, -d) if d else block)

    proj = mixer_proj
    mixer_in = lax.all_gather(gated, "tp", axis=0, tiled=True)
    for c, own in enumerate(chunks):
        part_in = lax.all_gather(own, "tp", axis=1, tiled=True)
        hidden = expert_hidden(part_in, scale_of(squares_of(part_in)), gate_weight, up_weight)
        outs.append(
            lax.psum_scatter(
                product(hidden, down_weight), "tp", scatter_dimension=1, tiled=True
            )
        )
        send_back(c)

    returned = jnp.concatenate(returned, axis=0)
    weights = sum(
        jnp.where(slots[None, :] == places[k][:, None], route_weights[:, k][:, None], 0.0)
        for k in range(2)
    )
    high = weights.astype(jnp.bfloat16)
    low = (weights - high.astype(jnp.float32)).astype(jnp.bfloat16)
    both = jnp.dot(
        jnp.concatenate([high, low], axis=0), returned, preferred_element_type=jnp.float32
    )
    expert_out = (both[:rows_b] + both[rows_b:]).astype(jnp.bfloat16)

    mixed_out = lax.dot_general(
        mixer_in, proj, (((0,), (0,)), ((), ())), preferred_element_type=jnp.float32
    ).astype(jnp.bfloat16)
    return (mixed_out, expert_out)


def body(*args):
    square = lax.axis_size("tp") == 4 and lax.axis_size("ep") == 8
    return fused(*args) if square else general(*args)


def solution(mesh):
    return jax.shard_map(
        body,
        mesh=mesh,
        in_specs=(
            P("tp", "ep"),
            P("tp", "ep"),
            P("tp", "ep"),
            P(),
            P(None, "tp"),
            P("ep", "tp"),
            P("ep", None),
            P("ep", None),
            P("ep", None, "tp"),
            P("ep", None, "tp"),
            P("ep", "tp", None),
        ),
        out_specs=(P("ep", "tp"), P("ep", "tp")),
        check_vma=False,
    )
```

```python
import functools

import jax
import jax.numpy as jnp
from jax import lax
from jax.experimental import pallas as pl
from jax.experimental.pallas import tpu as pltpu
from jax.sharding import PartitionSpec as P

KERNEL = 3
EPSILON = 1e-06
LANES = 128
CHUNKS = 16
TILE = 2
PIECES = 2
EARLY = 5
MIDDLE = 3
COUNTS = ((3, 2, 2), (2, 2, 2), (2, 2, 2), (2, 1, 0))
LATER = (0, 2)
EARLY_PART = (5, 8)


def metering():
    at, lows, highs = EARLY + MIDDLE, [[], [], []], [[], [], []]
    for counts in COUNTS:
        for slot, count in enumerate(counts):
            lows[slot].append(at)
            at += count
            highs[slot].append(at)
    late = [at]
    for count in LATER:
        late.append(late[-1] + count)
    return list(zip(lows, highs)), late


METER, LATE = metering()
MESH = pl.DeviceIdType.MESH


def pick(index, values):
    out = jnp.int32(values[-1])
    for i in range(len(values) - 1):
        out = jnp.where(index == i, jnp.int32(values[i]), out)
    return out


def aligned(start, size):
    return pl.ds(pl.multiple_of(start, size), size)


def fused_kernel(
    early_rows,
    conv_input, out_gate, in_gate, taps, proj_in, tokens, routes, weights, gate_in, up_in, down_in,
    mixed_out, expert_out,
    x, wg, wu, wd, cin, cig, cog, zb, y, proj, tap_buf, tap_in, route_buf, weight_buf,
    tabs, wcols, hidden, part_out, part_in, sums, fold, one, two_out, two_in, tot, tot_in, mixed, final,
    load_sem, s_xy, r_xy, s_z, r_z, s_pc, r_pc, s_tab, r_tab, s_rim, r_rim, s_mix, r_mix,
    s_part, r_part, s_fold, r_fold, s_one, r_one, s_two, r_two, s_tot, r_tot, out_sem,
):
    rows, part = tokens.shape
    blocks = x.shape[0] // rows
    levels = blocks // 2
    features = x.shape[1]
    units = wg.shape[1]
    width, length = conv_input.shape
    step = length // CHUNKS
    wide = step * TILE
    tiles_of = CHUNKS // TILE
    half = rows // 2
    ep, here = lax.axis_index("ep"), lax.axis_index("tp")
    level, core = ep // 2, ep % 2
    end = (level == 0) | (level == levels - 1)

    def device(level_to, core_to, tp_to):
        return {"ep": level_to * 2 + core_to, "tp": tp_to}

    xn, yn = device(level, core, here ^ 1), device(level, core, here ^ 2)
    pc = device(level, 1 - core, here)

    def remote(src, dst, send_sem, recv_sem, target):
        return pltpu.make_async_remote_copy(
            src_ref=src, dst_ref=dst, send_sem=send_sem, recv_sem=recv_sem,
            device_id=target, device_id_type=MESH,
        )

    def each(begin, stop, action):
        def run(i, carry):
            action(i)
            return carry

        lax.fori_loop(begin, stop, run, 0)

    def order(k):
        return pick(level * 4 + k, [1, 2, 3, 0, 2, 0, 3, 1, 1, 3, 0, 2, 2, 1, 0, 3])

    barrier = pltpu.get_barrier_semaphore()
    for target in [xn, yn, pc]:
        pl.semaphore_signal(barrier, inc=1, device_id=target, device_id_type=MESH)
    for away in range(1, levels):
        pl.semaphore_signal(
            barrier, inc=1, device_id=device((level + away) % levels, core, here),
            device_id_type=MESH,
        )
    has_next, has_prev = ep < blocks - 1, ep > 0
    far_rim = ((core == 1) & has_next) | ((core == 0) & has_prev)
    rim_ep = jnp.where(core == 1, ep + 1, ep - 1)

    @pl.when(far_rim)
    def _():
        pl.semaphore_signal(
            barrier, inc=1, device_id={"ep": rim_ep, "tp": here}, device_id_type=MESH
        )

    def block_rows(level_of, core_of, begin=0, size=None):
        size = rows if size is None else size
        return pl.ds(pl.multiple_of((level_of * 2 + core_of) * rows + begin, 16), size)

    def cols(relative):
        return aligned((here ^ relative) * part, part)

    own_at = x.at[block_rows(level, core), cols(0)]
    loads = [
        (routes, route_buf), (weights, weight_buf), (taps, tap_in), (tokens, own_at),
        (conv_input, cin), (in_gate, cig), (out_gate, cog), (gate_in, wg), (up_in, wu),
        (down_in, wd), (proj_in, proj),
    ]
    loads = [
        pltpu.make_async_copy(src, dst, load_sem.at[i]) for i, (src, dst) in enumerate(loads)
    ]
    for copy in loads:
        copy.start()

    names = lax.broadcasted_iota(jnp.int32, (blocks, rows), 0)
    for copy in loads[:3]:
        copy.wait()
    table = jnp.zeros((blocks, rows), jnp.float32)
    for k in range(2):
        table = table + jnp.where(route_buf[k : k + 1, :] == names, weight_buf[k : k + 1, :], 0.0)
    tabs[ep] = table
    tap_buf[...] = jnp.zeros_like(tap_buf)
    tap_buf[0:KERNEL, :] = tap_in[:, aligned(here * width, width)]
    tap_cols = jnp.transpose(tap_buf[...])
    wcols[...] = jnp.zeros_like(wcols)

    for copy in loads[4:6]:
        copy.wait()

    def make_z(q):
        at = aligned(q * wide, wide)
        value = cin[:, at].astype(jnp.float32) * cig[:, at].astype(jnp.float32)
        zb[:, pl.ds(pl.multiple_of(q * wide + LANES, LANES), wide)] = value.astype(jnp.bfloat16)

    with jax.named_scope("barrier"):
        make_z(tiles_of - 1)
        loads[3].wait()
        pl.semaphore_wait(barrier, 2 + levels + far_rim.astype(jnp.int32))

    def plane(level_of, way, low):
        size = rows - low
        lower = (size // 2 + 15) // 16 * 16
        begin, count, relative, target = (
            (low, size, 0, xn), (low, size, 0, yn),
            (low, lower, 1, yn), (low + lower, size - lower, 2, xn),
        )[way]
        at = x.at[block_rows(level_of, core, begin, count), cols(relative)]
        sem = level_of * 4 + way
        return remote(at, at, s_xy.at[sem], r_xy.at[sem], target)

    def along(level_of, relative, up):
        at = x.at[
            block_rows(level_of, core, 0, rows if relative == 0 else early_rows), cols(relative)
        ]
        side = level_of * 8 + relative * 2 + jnp.where(up, 1, 0)
        target = device(jnp.where(up, level + 1, level - 1), core, here)
        return remote(at, at, s_z.at[side], r_z.at[level_of * 4 + relative], target)

    def partner(level_of, relative):
        at = x.at[block_rows(level_of, core), cols(relative)]
        sem = level_of * 4 + relative
        return remote(at, at, s_pc.at[sem], r_pc.at[sem], pc)

    def spread(relative):
        @pl.when(level < levels - 1)
        def _():
            along(level, relative, True).start()

        @pl.when(level > 0)
        def _():
            along(level, relative, False).start()

    def table_to(away):
        target = device((level + away) % levels, core, here)
        return remote(tabs.at[ep], tabs.at[ep], s_tab.at[away], r_tab.at[ep], target)

    def table_pc(level_of):
        at = tabs.at[level_of * 2 + core]
        return remote(at, at, s_tab.at[levels + level_of], r_tab.at[level_of * 2 + core], pc)

    def table_wait(block):
        at = tabs.at[block]
        remote(at, at, s_tab.at[0], r_tab.at[block], pc).wait_recv()

    rim_copy = remote(
        zb.at[:, pl.ds(length, LANES)], zb.at[:, pl.ds(0, LANES)], s_rim, r_rim,
        {"ep": jnp.where(has_next, ep + 1, ep), "tp": here},
    )

    spread(0)
    plane(level, 0, 0).start()
    plane(level, 1, 0).start()
    partner(level, 0).start()

    @pl.when(has_next)
    def _():
        rim_copy.start()

    for away in range(1, levels):
        table_to(away).start()
    table_pc(level).start()

    with jax.named_scope("make_z"):
        each(0, tiles_of - 1, make_z)
        loads[6].wait()

    own_channels = aligned(here * width, width)

    def conv_chunk(q):
        at = aligned(q * wide, wide)
        value = zb[:, pl.ds(pl.multiple_of(q * wide, LANES), wide + LANES)].astype(jnp.float32)
        total = jnp.zeros((width, wide), jnp.float32)
        for lag in range(KERNEL):
            moved = pltpu.roll(value, lag, 1) if lag else value
            total = total + tap_cols[:, lag : lag + 1] * moved[:, LANES:]
        y[own_channels, at] = (cog[:, at].astype(jnp.float32) * total).astype(jnp.bfloat16)

    with jax.named_scope("conv"):
        each(1, tiles_of, conv_chunk)

    @pl.when(has_prev)
    def _():
        rim_copy.wait_recv()

    @pl.when(jnp.logical_not(has_prev))
    def _():
        zb[:, 0:LANES] = jnp.zeros((width, LANES), jnp.bfloat16)

    conv_chunk(0)

    def mix(q, way):
        at = aligned(q * step, step)
        if way < 2:
            src, target = y.at[own_channels, at], (xn, yn)[way]
            sem = q * 3 + way
        else:
            src = y.at[aligned((here ^ way // 2) * width, width), at]
            target = {2: yn, 4: xn}[way]
            sem = q * 3 + 2
        return remote(src, src, s_mix.at[sem], r_mix.at[sem], target)

    def mix_event(n):
        @pl.when(n < CHUNKS)
        def _():
            mix(n, 0).start()
            mix(n, 1).start()

        @pl.when(n >= CHUNKS)
        def _():
            q = n - CHUNKS

            @pl.when(q % 2 == 0)
            def _():
                mix(q, 0).wait_recv()
                mix(q, 2).start()

            @pl.when(q % 2 == 1)
            def _():
                mix(q, 1).wait_recv()
                mix(q, 4).start()

    def pass_on(k, relative):
        from_level = order(k)
        up = from_level < level
        relay = jnp.where(up, level < levels - 1, level > 0)

        @pl.when(relay)
        def _():
            along(from_level, relative, up).start()

    def arrive(k, relative):
        from_level = order(k)
        along(from_level, relative, from_level < level).wait_recv()
        pass_on(k, relative)
        return from_level

    def first_event(k, now=True):
        if now:
            from_level = arrive(k, 0)
        else:
            from_level = order(k)
            along(from_level, 0, from_level < level).wait_recv()
        plane(from_level, 0, early_rows).start()
        plane(from_level, 1, early_rows).start()
        partner(from_level, 0).start()

    def second_event(k):
        from_level = arrive(k, 1)
        plane(from_level, 0, early_rows).wait_recv()
        plane(from_level, 2, early_rows).start()
        partner(from_level, 1).start()

    def third_event(k):
        from_level = arrive(k, 2)
        plane(from_level, 1, early_rows).wait_recv()
        plane(from_level, 3, early_rows).start()
        partner(from_level, 2).start()

    def fourth_event(k):
        from_level = arrive(k, 3)
        plane(from_level, 2, early_rows).wait_recv()
        plane(from_level, 3, early_rows).wait_recv()
        partner(from_level, 3).start()

    with jax.named_scope("own_plane"):
        plane(level, 0, 0).wait_recv()
        plane(level, 2, 0).start()
        spread(1)
        partner(level, 1).start()
        plane(level, 1, 0).wait_recv()
        plane(level, 3, 0).start()
        spread(2)
        partner(level, 2).start()
    near = jnp.where(end, 1, 2)
    each(0, near, lambda k: first_event(k, now=False))
    with jax.named_scope("own_far"):
        for away in range(1, levels):
            other = (level + away) % levels
            table_wait(other * 2 + core)
            table_pc(other).start()
        each(0, EARLY, mix_event)
        plane(level, 2, 0).wait_recv()
        plane(level, 3, 0).wait_recv()
    spread(3)
    partner(level, 3).start()
    each(0, near, lambda k: pass_on(k, 0))
    for slot, edge in ((0, 0), (1, levels - 1)):
        @pl.when(level == edge)
        def _():
            fold[slot] = jnp.zeros(fold.shape[1:], jnp.bfloat16)

    for source in range(levels):
        @pl.when((source == level + 1) | (source == level - 1))
        def _():
            tot_in[source] = jnp.zeros(tot_in.shape[1:], jnp.bfloat16)

    with jax.named_scope("near_23"):
        each(0, near, second_event)
        each(0, near, third_event)
    each(EARLY, EARLY + MIDDLE, mix_event)
    for away in range(levels):
        table_wait((level + away) % levels * 2 + 1 - core)
    for block in range(blocks):
        wcols_at = tabs[block, pl.ds(ep, 1), :]
        tap_buf[block : block + 1, :] = wcols_at
    wcols[...] = jnp.transpose(tap_buf[...])
    with jax.named_scope("near_4"):
        each(0, near, fourth_event)
    def one_copy(k, relative, axis):
        begin = 0 if axis == 0 else half
        at = sums.at[k, relative, pl.ds(begin, half)]
        slot = {(1, 0): 0, (3, 0): 1, (2, 1): 0, (3, 1): 1}[relative, axis]
        sem = (k * 2 + axis) * 2 + slot
        return remote(at, one.at[k, axis, slot], s_one.at[sem], r_one.at[sem], (xn, yn)[axis])

    def two_copy(k, axis):
        sem = k * 2 + axis
        return remote(
            two_out.at[k, axis], two_in.at[k, axis], s_two.at[sem], r_two.at[sem], (yn, xn)[axis]
        )

    def total_copy(k):
        to = order(k)
        return remote(
            tot.at[k], tot_in.at[level], s_tot.at[k], r_tot.at[level], device(to, core, here)
        )

    def part_copy(k, relative):
        sem = k * 4 + relative
        return remote(
            part_out.at[k, relative], part_in.at[k, relative], s_part.at[sem], r_part.at[sem], pc
        )

    def fold_copy(k, relative):
        to = order(k)
        slot = jnp.where(to > level, 0, 1)
        sem = slot * 4 + relative
        return remote(
            sums.at[k, relative], fold.at[slot, relative], s_fold.at[sem], r_fold.at[sem],
            device(to, core, here),
        )

    def fold_wait(slot, relative):
        at = fold.at[slot, relative]
        remote(at, at, s_fold.at[0], r_fold.at[slot * 4 + relative], xn).wait_recv()

    def second_stage(k):
        for axis, relative in ((0, 2), (1, 1)):
            begin = 0 if axis == 0 else half
            one_copy(k, (1, 2)[axis], axis).wait_recv()
            one_copy(k, 3, axis).wait_recv()
            two_out[k, axis] = (
                sums[k, relative, begin : begin + half].astype(jnp.float32)
                + one[k, axis, 1].astype(jnp.float32)
            ).astype(jnp.bfloat16)
            two_copy(k, axis).start()

    def third_stage(k):
        to = order(k)
        for axis in range(2):
            begin = 0 if axis == 0 else half
            two_copy(k, axis).wait_recv()
            tot[k, begin : begin + half] = (
                sums[k, 0, begin : begin + half].astype(jnp.float32)
                + one[k, axis, 0].astype(jnp.float32)
                + two_in[k, axis].astype(jnp.float32)
            ).astype(jnp.bfloat16)

        @pl.when(to != level)
        def _():
            total_copy(k).start()

        @pl.when(to == level)
        def _():
            tot_in[level] = tot[k]

    def column_of(block):
        lane = lax.broadcasted_iota(jnp.int32, (rows, LANES), 1)
        return jnp.sum(jnp.where(lane == block, wcols[...], 0.0), axis=1, keepdims=True)

    tile = min(256, units)

    def iteration(k):
        from_level = order(k)

        begin = jnp.minimum(near + k, 3)
        stop = jnp.minimum(near + k + 1, 3)

        def mixes(lows, highs):
            with jax.named_scope("mix_ev"):
                each(pick(k, lows), pick(k, highs), mix_event)

        with jax.named_scope("pc_wait"):
            for relative in range(4):
                at = x.at[block_rows(from_level, 1 - core), cols(relative)]
                remote(
                    at, at, s_pc.at[0], r_pc.at[from_level * 4 + relative], pc
                ).wait_recv()

        pair = pl.ds(pl.multiple_of(from_level * 2 * rows, 2 * rows), 2 * rows)
        squares = jnp.zeros((2 * rows, LANES), jnp.float32)
        for first in range(0, features, LANES):
            value = x[pair, first : first + LANES].astype(jnp.float32)
            squares = squares + value * value
        scale = lax.rsqrt(jnp.sum(squares, axis=1, keepdims=True) / features + EPSILON)

        def hidden_tile(n):
            at = aligned(n * tile, tile)
            rows_in = x[pair, :]
            gate = scale * jnp.dot(rows_in, wg[:, at], preferred_element_type=jnp.float32)
            up = scale * jnp.dot(rows_in, wu[:, at], preferred_element_type=jnp.float32)
            hidden[:, at] = (gate / (1.0 + jnp.exp(-gate)) * up).astype(jnp.bfloat16)

        tiles = units // tile

        with jax.named_scope("hidden"):
            each(0, tiles // 2, hidden_tile)
        with jax.named_scope("third_stage"):
            @pl.when(k >= near + 2)
            def _():
                third_stage(k - 2)

        with jax.named_scope("event_a"):
            each(begin, stop, first_event)
        mixes(*METER[0])
        with jax.named_scope("hidden"):
            each(tiles // 2, tiles, hidden_tile)
        mixes(*METER[1])

        def product(core_of, relative):
            value = hidden[aligned(core_of * rows, rows), :]
            weight = wd[:, cols(relative)]
            return column_of(from_level * 2 + core_of) * jnp.dot(
                value, weight, preferred_element_type=jnp.float32
            )

        with jax.named_scope("down_out"):
            for relative in (3, 1, 2, 0):
                part_out[k, relative] = product(1 - core, relative).astype(jnp.bfloat16)
                part_copy(k, relative).start()
        with jax.named_scope("second_stage"):
            @pl.when(k >= near + 1)
            def _():
                second_stage(k - 1)

        with jax.named_scope("event_c"):
            each(begin, stop, second_event)
            each(begin, stop, third_event)
        mixes(*METER[2])
        with jax.named_scope("down_own"):
            for relative in (3, 1, 2, 0):
                value = product(core, relative)
                part_copy(k, relative).wait_recv()
                value = value + part_in[k, relative].astype(jnp.float32)

                @pl.when(k < levels - 1)
                def _():
                    sums[k, relative] = value.astype(jnp.bfloat16)

                @pl.when(k == levels - 1)
                def _():
                    @pl.when(level > 0)
                    def _():
                        fold_wait(0, relative)

                    @pl.when(level < levels - 1)
                    def _():
                        fold_wait(1, relative)

                    sums[k, relative] = (
                        value
                        + fold[0, relative].astype(jnp.float32)
                        + fold[1, relative].astype(jnp.float32)
                    ).astype(jnp.bfloat16)

                @pl.when(k < near)
                def _():
                    fold_copy(k, relative).start()

                @pl.when(k >= near)
                def _():
                    for axis in range(2):
                        if relative in (3, axis + 1):
                            one_copy(k, relative, axis).start()

        with jax.named_scope("event_d"):
            each(begin, stop, fourth_event)

    with jax.named_scope("weights_wait"):
        for copy in loads[7:]:
            copy.wait()

    each(0, levels, iteration)

    def mix_tile(q):
        for piece in range(TILE):
            mix(q * TILE + piece, 1 - piece % 2).wait_recv()
            mix(q * TILE + piece, 2).wait_recv()
        at = aligned(q * wide, wide)
        mixed[at, :] = lax.dot_general(
            y[:, at], proj[...], (((0,), (0,)), ((), ())), preferred_element_type=jnp.float32
        ).astype(jnp.bfloat16)
        pltpu.make_async_copy(mixed.at[at], mixed_out.at[at], out_sem.at[q]).start()

    each(LATE[0], LATE[1], mix_event)
    with jax.named_scope("mix_tiles"):
        each(0, tiles_of // 4, mix_tile)
    with jax.named_scope("last_third"):
        third_stage(levels - 2)
    each(LATE[1], LATE[2], mix_event)
    with jax.named_scope("mix_tiles"):
        each(tiles_of // 4, tiles_of // 2, mix_tile)
    with jax.named_scope("last_second"):
        second_stage(levels - 1)
    each(LATE[2], 2 * CHUNKS, mix_event)
    with jax.named_scope("mix_tiles"):
        each(tiles_of // 2, tiles_of, mix_tile)
    with jax.named_scope("last_third"):
        third_stage(levels - 1)
    with jax.named_scope("tot_wait"):
        for away in range(1, levels):
            source = (level + away) % levels

            @pl.when((source > level + 1) | (source < level - 1))
            def _():
                at = tot_in.at[source]
                remote(at, at, s_tot.at[0], r_tot.at[source], xn).wait_recv()
    answer = jnp.zeros((rows, part), jnp.float32)
    for source in range(levels):
        answer = answer + tot_in[source].astype(jnp.float32)
    final[...] = answer.astype(jnp.bfloat16)
    last = pltpu.make_async_copy(final, expert_out, out_sem.at[CHUNKS])
    last.start()

    with jax.named_scope("finish"):
        for relative in range(4):
            @pl.when(level < levels - 1)
            def _():
                along(level, relative, True).wait_send()

            @pl.when(level > 0)
            def _():
                along(level, relative, False).wait_send()

            partner(level, relative).wait_send()
            plane(level, relative, 0).wait_send()

        @pl.when(has_next)
        def _():
            rim_copy.wait_send()

        for away in range(1, levels):
            table_to(away).wait_send()
        for level_of in range(levels):
            table_pc(level_of).wait_send()

        def finish(k):
            from_level = order(k)
            up = from_level < level
            relay = jnp.where(up, level < levels - 1, level > 0)
            for relative in range(4):
                @pl.when((k < levels - 1) & relay)
                def _():
                    along(from_level, relative, up).wait_send()

                @pl.when(k < levels - 1)
                def _():
                    plane(from_level, relative, early_rows).wait_send()
                    partner(from_level, relative).wait_send()

                part_copy(k, relative).wait_send()

                @pl.when(k < near)
                def _():
                    fold_copy(k, relative).wait_send()

            @pl.when(k >= near)
            def _():
                for axis in range(2):
                    one_copy(k, axis + 1, axis).wait_send()
                    one_copy(k, 3, axis).wait_send()
                    two_copy(k, axis).wait_send()

            @pl.when((from_level != level) & (k >= near))
            def _():
                total_copy(k).wait_send()

        each(0, levels, finish)

        def finish_mix(q):
            for way in range(3):
                mix(q, way).wait_send()

        def finish_out(q):
            at = aligned(q * wide, wide)
            pltpu.make_async_copy(mixed.at[at], mixed_out.at[at], out_sem.at[q]).wait()

        each(0, CHUNKS, finish_mix)
        each(0, tiles_of, finish_out)
        last.wait()


def fused(*args):
    (conv_input, out_gate, in_gate, conv_taps, mixer_proj, token_rows, routes, route_weights,
     expert_gate, expert_up, expert_down) = args
    tp, experts = lax.axis_size("tp"), lax.axis_size("ep")
    rows, part = token_rows.shape
    features = part * tp
    units = expert_gate.shape[2]
    width, length = conv_input.shape
    levels, half = experts // 2, rows // 2
    early_rows = rows * EARLY_PART[0] // EARLY_PART[1] // 16 * 16
    bf16, f32 = jnp.bfloat16, jnp.float32
    dma = pltpu.SemaphoreType.DMA
    hold = pltpu.VMEM
    scratch = [
        hold((experts * rows, features), bf16),
        hold((features, units), bf16), hold((features, units), bf16), hold((units, features), bf16),
        hold((width, length), bf16), hold((width, length), bf16), hold((width, length), bf16),
        hold((width, length + LANES), bf16),
        hold((tp * width, length), bf16),
        hold(mixer_proj.shape, bf16),
        hold((LANES, max(width, rows)), f32),
        hold(conv_taps.shape, f32),
        hold((2, rows), jnp.int32), hold((2, rows), f32),
        hold((experts, experts, rows), f32),
        hold((rows, LANES), f32),
        hold((2 * rows, units), bf16),
        hold((levels, 4, rows, part), bf16), hold((levels, 4, rows, part), bf16),
        hold((levels, 4, rows, part), bf16),
        hold((2, 4, rows, part), bf16),
        hold((levels, 2, 2, half, part), bf16),
        hold((levels, 2, half, part), bf16), hold((levels, 2, half, part), bf16),
        hold((levels, rows, part), bf16), hold((levels, rows, part), bf16),
        hold((length, part), bf16),
        hold((rows, part), bf16),
        dma((11,)),
        dma((levels * 4,)), dma((levels * 4,)),
        dma((levels * 8,)), dma((levels * 4,)),
        dma((levels * 4,)), dma((levels * 4,)),
        dma((levels * 2,)), dma((experts,)),
        dma, dma,
        dma((CHUNKS * 3,)), dma((CHUNKS * 3,)),
        dma((levels * 4,)), dma((levels * 4,)),
        dma((8,)), dma((8,)),
        dma((levels * 4,)), dma((levels * 4,)),
        dma((levels * 2,)), dma((levels * 2,)),
        dma((levels,)), dma((levels,)),
        dma((CHUNKS + 1,)),
    ]
    anywhere = pl.BlockSpec(memory_space=pl.ANY)
    return pl.pallas_call(
        functools.partial(fused_kernel, early_rows),
        out_shape=(
            jax.ShapeDtypeStruct((length, part), bf16), jax.ShapeDtypeStruct((rows, part), bf16)
        ),
        in_specs=[anywhere] * 11,
        out_specs=(anywhere, anywhere),
        scratch_shapes=scratch,
        compiler_params=pltpu.CompilerParams(
            collective_id=0, has_side_effects=True, vmem_limit_bytes=67043328
        ),
    )(
        conv_input, out_gate, in_gate, conv_taps, mixer_proj, token_rows, routes.T,
        route_weights.T, expert_gate[0], expert_up[0], expert_down[0],
    )


def passed_along(value, axis, by):
    devices = lax.axis_size(axis)
    pairs = [(i, i + by) for i in range(devices) if 0 <= i + by < devices]
    return lax.ppermute(value, axis, pairs)


def rotated(value, by):
    devices = lax.axis_size("ep")
    return lax.ppermute(value, "ep", [(i, (i + by) % devices) for i in range(devices)])


def routing(route_ids, capacity, experts):
    rows = route_ids.shape[0]
    names = jnp.arange(experts, dtype=jnp.int32)[None, :]
    hits = [(route_ids[:, k][:, None] == names) for k in range(2)]
    both = (hits[0] | hits[1]).astype(jnp.bfloat16)
    index = jnp.arange(rows, dtype=jnp.int32)
    lower = (index[:, None] > index[None, :]).astype(jnp.bfloat16)
    earlier = jnp.dot(lower, both, preferred_element_type=jnp.float32)
    away = lax.rem(route_ids - lax.axis_index("ep") + experts, experts)
    places = []
    for k in range(2):
        rank = jnp.sum(jnp.where(hits[k], earlier, 0.0), axis=1).astype(jnp.int32)
        places.append(away[:, k] * capacity + rank)
    return places


def expert_hidden(part_in, row_scale, gate_weight, up_weight):
    gate_sum = jnp.dot(part_in, gate_weight, preferred_element_type=jnp.float32)
    up_sum = jnp.dot(part_in, up_weight, preferred_element_type=jnp.float32)
    return (jax.nn.silu(row_scale * gate_sum) * (row_scale * up_sum)).astype(jnp.bfloat16)


def product(hidden, down):
    return jnp.dot(hidden, down, preferred_element_type=jnp.float32).astype(jnp.bfloat16)


def general(
    conv_input,
    out_gate,
    in_gate,
    conv_taps,
    mixer_proj,
    token_rows,
    routes,
    route_weights,
    expert_gate,
    expert_up,
    expert_down,
):
    tp = lax.axis_size("tp")
    here = lax.axis_index("tp")
    width_part = conv_input.shape[0]
    length = conv_input.shape[1]
    local_taps = lax.dynamic_slice_in_dim(conv_taps, here * width_part, width_part, 1)

    experts = lax.axis_size("ep")
    rows_b, cols_part = token_rows.shape
    capacity = 4 * rows_b // experts
    slot_total = experts * capacity
    feature_count = cols_part * tp
    places = routing(routes, capacity, experts)
    slots = jnp.arange(slot_total, dtype=jnp.int32)
    picks = [(slots[:, None] == places[k][None, :]) for k in range(2)]
    chosen = (picks[0] | picks[1]).astype(jnp.bfloat16)
    buffer = jnp.dot(chosen, token_rows, preferred_element_type=jnp.float32).astype(jnp.bfloat16)

    z_rows = (conv_input.astype(jnp.float32) * in_gate.astype(jnp.float32)).astype(jnp.bfloat16)
    rim_rows = passed_along(z_rows[:, length - (KERNEL - 1) :], "ep", 1)
    longer = jnp.concatenate([rim_rows, z_rows], axis=1).astype(jnp.float32)
    conv_sum = jnp.zeros(z_rows.shape, jnp.float32)
    for lag_index in range(KERNEL):
        begin = KERNEL - 1 - lag_index
        conv_sum = conv_sum + local_taps[lag_index][:, None] * longer[:, begin : begin + length]
    gated = (out_gate.astype(jnp.float32) * conv_sum).astype(jnp.bfloat16)

    gated, buffer = lax.optimization_barrier((gated, buffer))
    arrived = [
        rotated(buffer[d * capacity : (d + 1) * capacity], d) if d else buffer[:capacity]
        for d in range(experts)
    ]
    chunk_parts = experts // PIECES
    chunks = [
        jnp.concatenate(arrived[c * chunk_parts : (c + 1) * chunk_parts], axis=0)
        for c in range(PIECES)
    ]
    gate_weight, up_weight, down_weight = expert_gate[0], expert_up[0], expert_down[0]

    def squares_of(part_in):
        return jnp.sum(jnp.square(part_in.astype(jnp.float32)), axis=1)

    def scale_of(squares):
        return lax.rsqrt(squares / feature_count + EPSILON)[:, None]

    outs, returned = [], []

    def send_back(c):
        for i in range(chunk_parts):
            d = c * chunk_parts + i
            block = outs[c][i * capacity : (i + 1) * capacity]
            returned.append(rotated(block, -d) if d else block)

    proj = mixer_proj
    mixer_in = lax.all_gather(gated, "tp", axis=0, tiled=True)
    for c, own in enumerate(chunks):
        part_in = lax.all_gather(own, "tp", axis=1, tiled=True)
        hidden = expert_hidden(part_in, scale_of(squares_of(part_in)), gate_weight, up_weight)
        outs.append(
            lax.psum_scatter(
                product(hidden, down_weight), "tp", scatter_dimension=1, tiled=True
            )
        )
        send_back(c)

    returned = jnp.concatenate(returned, axis=0)
    weights = sum(
        jnp.where(slots[None, :] == places[k][:, None], route_weights[:, k][:, None], 0.0)
        for k in range(2)
    )
    high = weights.astype(jnp.bfloat16)
    low = (weights - high.astype(jnp.float32)).astype(jnp.bfloat16)
    both = jnp.dot(
        jnp.concatenate([high, low], axis=0), returned, preferred_element_type=jnp.float32
    )
    expert_out = (both[:rows_b] + both[rows_b:]).astype(jnp.bfloat16)

    mixed_out = lax.dot_general(
        mixer_in, proj, (((0,), (0,)), ((), ())), preferred_element_type=jnp.float32
    ).astype(jnp.bfloat16)
    return (mixed_out, expert_out)


def body(*args):
    square = lax.axis_size("tp") == 4 and lax.axis_size("ep") == 8
    return fused(*args) if square else general(*args)


def solution(mesh):
    return jax.shard_map(
        body,
        mesh=mesh,
        in_specs=(
            P("tp", "ep"),
            P("tp", "ep"),
            P("tp", "ep"),
            P(),
            P(None, "tp"),
            P("ep", "tp"),
            P("ep", None),
            P("ep", None),
            P("ep", None, "tp"),
            P("ep", None, "tp"),
            P("ep", "tp", None),
        ),
        out_specs=(P("ep", "tp"), P("ep", "tp")),
        check_vma=False,
    )
```

```python
import functools

import jax
import jax.numpy as jnp
from jax import lax
from jax.experimental import pallas as pl
from jax.experimental.pallas import tpu as pltpu
from jax.sharding import PartitionSpec as P

KERNEL = 3
EPSILON = 1e-06
LANES = 128
CHUNKS = 16
TILE = 2
PIECES = 2
COPIES = 8
EARLY = 2
MIDDLE = 6
COUNTS = ((3, 1, 3), (2, 1, 6), (2, 2, 0), (2, 0, 0))
LATER = (0, 2)
EARLY_PART = (5, 8)


def metering():
    at, lows, highs = EARLY + MIDDLE, [[], [], []], [[], [], []]
    for counts in COUNTS:
        for slot, count in enumerate(counts):
            lows[slot].append(at)
            at += count
            highs[slot].append(at)
    late = [at]
    for count in LATER:
        late.append(late[-1] + count)
    return list(zip(lows, highs)), late


METER, LATE = metering()
MESH = pl.DeviceIdType.MESH


def pick(index, values):
    out = jnp.int32(values[-1])
    for i in range(len(values) - 1):
        out = jnp.where(index == i, jnp.int32(values[i]), out)
    return out


def aligned(start, size):
    return pl.ds(pl.multiple_of(start, size), size)


def fused_kernel(
    early_rows,
    conv_input, out_gate, in_gate, taps, proj_in, tokens, routes, weights, gate_in, up_in, down_in,
    mixed_out, expert_out,
    x, wg, wu, wd, cin, cig, cog, zb, y, proj, tap_buf, tap_in, route_buf, weight_buf,
    tabs, wcols, hidden, part_out, part_in, sums, fold, one, two_out, two_in, tot, tot_in, mixed, final,
    load_sem, s_xy, r_xy, s_z, r_z, s_pc, r_pc, s_tab, r_tab, s_rim, r_rim, s_mix, r_mix,
    s_part, r_part, s_fold, r_fold, s_one, r_one, s_two, r_two, s_tot, r_tot, out_sem,
):
    rows, part = tokens.shape
    blocks = x.shape[0] // rows
    levels = blocks // 2
    features = x.shape[1]
    units = wg.shape[1]
    width, length = conv_input.shape
    step = length // CHUNKS
    wide = step * TILE
    tiles_of = CHUNKS // TILE
    half = rows // 2
    ep, here = lax.axis_index("ep"), lax.axis_index("tp")
    level, core = ep // 2, ep % 2
    end = (level == 0) | (level == levels - 1)

    def device(level_to, core_to, tp_to):
        return {"ep": level_to * 2 + core_to, "tp": tp_to}

    xn, yn = device(level, core, here ^ 1), device(level, core, here ^ 2)
    pc = device(level, 1 - core, here)

    def remote(src, dst, send_sem, recv_sem, target):
        return pltpu.make_async_remote_copy(
            src_ref=src, dst_ref=dst, send_sem=send_sem, recv_sem=recv_sem,
            device_id=target, device_id_type=MESH,
        )

    def each(begin, stop, action):
        def run(i, carry):
            action(i)
            return carry

        lax.fori_loop(begin, stop, run, 0)

    def order(k):
        return pick(level * 4 + k, [1, 2, 3, 0, 2, 0, 3, 1, 1, 3, 0, 2, 2, 1, 0, 3])

    barrier = pltpu.get_barrier_semaphore()
    for target in [xn, yn, pc]:
        pl.semaphore_signal(barrier, inc=1, device_id=target, device_id_type=MESH)
    for away in range(1, levels):
        pl.semaphore_signal(
            barrier, inc=1, device_id=device((level + away) % levels, core, here),
            device_id_type=MESH,
        )
    has_next, has_prev = ep < blocks - 1, ep > 0
    far_rim = ((core == 1) & has_next) | ((core == 0) & has_prev)
    rim_ep = jnp.where(core == 1, ep + 1, ep - 1)

    @pl.when(far_rim)
    def _():
        pl.semaphore_signal(
            barrier, inc=1, device_id={"ep": rim_ep, "tp": here}, device_id_type=MESH
        )

    def block_rows(level_of, core_of, begin=0, size=None):
        size = rows if size is None else size
        return pl.ds(pl.multiple_of((level_of * 2 + core_of) * rows + begin, 16), size)

    def cols(relative):
        return aligned((here ^ relative) * part, part)

    own_at = x.at[block_rows(level, core), cols(0)]
    loads = [
        (routes, route_buf), (weights, weight_buf), (taps, tap_in), (tokens, own_at),
        (conv_input, cin), (in_gate, cig), (out_gate, cog), (gate_in, wg), (up_in, wu),
        (down_in, wd), (proj_in, proj),
    ]
    loads = [
        pltpu.make_async_copy(src, dst, load_sem.at[i]) for i, (src, dst) in enumerate(loads)
    ]
    for copy in loads:
        copy.start()

    names = lax.broadcasted_iota(jnp.int32, (blocks, rows), 0)
    for copy in loads[:3]:
        copy.wait()
    table = jnp.zeros((blocks, rows), jnp.float32)
    for k in range(2):
        table = table + jnp.where(route_buf[k : k + 1, :] == names, weight_buf[k : k + 1, :], 0.0)
    tabs[ep] = table
    tap_buf[...] = jnp.zeros_like(tap_buf)
    tap_buf[0:KERNEL, :] = tap_in[:, aligned(here * width, width)]
    tap_cols = jnp.transpose(tap_buf[...])
    wcols[...] = jnp.zeros_like(wcols)

    for copy in loads[4:6]:
        copy.wait()

    def make_z(q):
        at = aligned(q * wide, wide)
        value = cin[:, at].astype(jnp.float32) * cig[:, at].astype(jnp.float32)
        zb[:, pl.ds(pl.multiple_of(q * wide + LANES, LANES), wide)] = value.astype(jnp.bfloat16)

    with jax.named_scope("barrier"):
        make_z(tiles_of - 1)
        loads[3].wait()
        pl.semaphore_wait(barrier, 2 + levels + far_rim.astype(jnp.int32))

    def plane(level_of, way, low):
        size = rows - low
        lower = (size // 2 + 15) // 16 * 16
        begin, count, relative, target = (
            (low, size, 0, xn), (low, size, 0, yn),
            (low, lower, 1, yn), (low + lower, size - lower, 2, xn),
        )[way]
        at = x.at[block_rows(level_of, core, begin, count), cols(relative)]
        sem = level_of * 4 + way
        return remote(at, at, s_xy.at[sem], r_xy.at[sem], target)

    def along(level_of, relative, up):
        at = x.at[
            block_rows(level_of, core, 0, rows if relative == 0 else early_rows), cols(relative)
        ]
        side = level_of * 8 + relative * 2 + jnp.where(up, 1, 0)
        target = device(jnp.where(up, level + 1, level - 1), core, here)
        return remote(at, at, s_z.at[side], r_z.at[level_of * 4 + relative], target)

    def partner(level_of, relative):
        at = x.at[block_rows(level_of, core), cols(relative)]
        sem = level_of * 4 + relative
        return remote(at, at, s_pc.at[sem], r_pc.at[sem], pc)

    def spread(relative):
        @pl.when(level < levels - 1)
        def _():
            along(level, relative, True).start()

        @pl.when(level > 0)
        def _():
            along(level, relative, False).start()

    def table_to(away):
        target = device((level + away) % levels, core, here)
        return remote(tabs.at[ep], tabs.at[ep], s_tab.at[away], r_tab.at[ep], target)

    def table_pc(level_of):
        at = tabs.at[level_of * 2 + core]
        return remote(at, at, s_tab.at[levels + level_of], r_tab.at[level_of * 2 + core], pc)

    def table_wait(block):
        at = tabs.at[block]
        remote(at, at, s_tab.at[0], r_tab.at[block], pc).wait_recv()

    rim_copy = remote(
        zb.at[:, pl.ds(length, LANES)], zb.at[:, pl.ds(0, LANES)], s_rim, r_rim,
        {"ep": jnp.where(has_next, ep + 1, ep), "tp": here},
    )

    spread(0)
    plane(level, 0, 0).start()
    plane(level, 1, 0).start()
    partner(level, 0).start()

    @pl.when(has_next)
    def _():
        rim_copy.start()

    for away in range(1, levels):
        table_to(away).start()
    table_pc(level).start()

    with jax.named_scope("make_z"):
        each(0, tiles_of - 1, make_z)
        loads[6].wait()

    own_channels = aligned(here * width, width)

    def conv_chunk(q):
        at = aligned(q * wide, wide)
        value = zb[:, pl.ds(pl.multiple_of(q * wide, LANES), wide + LANES)].astype(jnp.float32)
        total = jnp.zeros((width, wide), jnp.float32)
        for lag in range(KERNEL):
            moved = pltpu.roll(value, lag, 1) if lag else value
            total = total + tap_cols[:, lag : lag + 1] * moved[:, LANES:]
        y[own_channels, at] = (cog[:, at].astype(jnp.float32) * total).astype(jnp.bfloat16)

    with jax.named_scope("conv"):
        each(1, tiles_of, conv_chunk)

    @pl.when(has_prev)
    def _():
        rim_copy.wait_recv()

    @pl.when(jnp.logical_not(has_prev))
    def _():
        zb[:, 0:LANES] = jnp.zeros((width, LANES), jnp.bfloat16)

    conv_chunk(0)

    def mix(q, way):
        at = aligned(q * step, step)
        if way < 2:
            src, target = y.at[own_channels, at], (xn, yn)[way]
            sem = q * 3 + way
        else:
            src = y.at[aligned((here ^ way // 2) * width, width), at]
            target = {2: yn, 4: xn}[way]
            sem = q * 3 + 2
        return remote(src, src, s_mix.at[sem], r_mix.at[sem], target)

    def mix_event(n):
        @pl.when(n < CHUNKS)
        def _():
            mix(n, 0).start()
            mix(n, 1).start()

        @pl.when(n >= CHUNKS)
        def _():
            q = n - CHUNKS

            @pl.when(q % 2 == 0)
            def _():
                mix(q, 0).wait_recv()
                mix(q, 2).start()

            @pl.when(q % 2 == 1)
            def _():
                mix(q, 1).wait_recv()
                mix(q, 4).start()

    def pass_on(k, relative):
        from_level = order(k)
        up = from_level < level
        relay = jnp.where(up, level < levels - 1, level > 0)

        @pl.when(relay)
        def _():
            along(from_level, relative, up).start()

    def arrive(k, relative):
        from_level = order(k)
        along(from_level, relative, from_level < level).wait_recv()
        pass_on(k, relative)
        return from_level

    def first_event(k, now=True):
        if now:
            from_level = arrive(k, 0)
        else:
            from_level = order(k)
            along(from_level, 0, from_level < level).wait_recv()
        plane(from_level, 0, early_rows).start()
        plane(from_level, 1, early_rows).start()
        partner(from_level, 0).start()

    def second_event(k):
        from_level = arrive(k, 1)
        plane(from_level, 0, early_rows).wait_recv()
        plane(from_level, 2, early_rows).start()
        partner(from_level, 1).start()

    def third_event(k):
        from_level = arrive(k, 2)
        plane(from_level, 1, early_rows).wait_recv()
        plane(from_level, 3, early_rows).start()
        partner(from_level, 2).start()

    def fourth_event(k):
        from_level = arrive(k, 3)
        plane(from_level, 2, early_rows).wait_recv()
        plane(from_level, 3, early_rows).wait_recv()
        partner(from_level, 3).start()

    with jax.named_scope("own_plane"):
        plane(level, 0, 0).wait_recv()
        plane(level, 2, 0).start()
        spread(1)
        partner(level, 1).start()
        plane(level, 1, 0).wait_recv()
        plane(level, 3, 0).start()
        spread(2)
        partner(level, 2).start()
    near = jnp.where(end, 1, 2)
    each(0, near, lambda k: first_event(k, now=False))
    with jax.named_scope("own_far"):
        for away in range(1, levels):
            other = (level + away) % levels
            table_wait(other * 2 + core)
            table_pc(other).start()
        each(0, EARLY, mix_event)
        plane(level, 2, 0).wait_recv()
        plane(level, 3, 0).wait_recv()
    spread(3)
    partner(level, 3).start()
    each(0, near, lambda k: pass_on(k, 0))
    for slot, edge in ((0, 0), (1, levels - 1)):
        @pl.when(level == edge)
        def _():
            fold[slot] = jnp.zeros(fold.shape[1:], jnp.bfloat16)

    for source in range(levels):
        @pl.when((source == level + 1) | (source == level - 1))
        def _():
            tot_in[source] = jnp.zeros(tot_in.shape[1:], jnp.bfloat16)

    with jax.named_scope("near_23"):
        each(0, near, second_event)
        each(0, near, third_event)
    each(EARLY, EARLY + MIDDLE, mix_event)
    for away in range(levels):
        table_wait((level + away) % levels * 2 + 1 - core)
    for block in range(blocks):
        wcols_at = tabs[block, pl.ds(ep, 1), :]
        tap_buf[block : block + 1, :] = wcols_at
    wcols[...] = jnp.transpose(tap_buf[...])
    with jax.named_scope("near_4"):
        each(0, near, fourth_event)
    def one_copy(k, relative, axis):
        begin = 0 if axis == 0 else half
        at = sums.at[k, relative, pl.ds(begin, half)]
        slot = {(1, 0): 0, (3, 0): 1, (2, 1): 0, (3, 1): 1}[relative, axis]
        sem = (k * 2 + axis) * 2 + slot
        return remote(at, one.at[k, axis, slot], s_one.at[sem], r_one.at[sem], (xn, yn)[axis])

    def two_copy(k, axis):
        sem = k * 2 + axis
        return remote(
            two_out.at[k, axis], two_in.at[k, axis], s_two.at[sem], r_two.at[sem], (yn, xn)[axis]
        )

    def total_copy(k):
        to = order(k)
        return remote(
            tot.at[k], tot_in.at[level], s_tot.at[k], r_tot.at[level], device(to, core, here)
        )

    def part_copy(k, relative):
        sem = k * 4 + relative
        return remote(
            part_out.at[k, relative], part_in.at[k, relative], s_part.at[sem], r_part.at[sem], pc
        )

    def fold_copy(k, relative):
        to = order(k)
        slot = jnp.where(to > level, 0, 1)
        sem = slot * 4 + relative
        return remote(
            sums.at[k, relative], fold.at[slot, relative], s_fold.at[sem], r_fold.at[sem],
            device(to, core, here),
        )

    def fold_wait(slot, relative):
        at = fold.at[slot, relative]
        remote(at, at, s_fold.at[0], r_fold.at[slot * 4 + relative], xn).wait_recv()

    def second_stage(k):
        for axis, relative in ((0, 2), (1, 1)):
            begin = 0 if axis == 0 else half
            one_copy(k, (1, 2)[axis], axis).wait_recv()
            one_copy(k, 3, axis).wait_recv()
            two_out[k, axis] = (
                sums[k, relative, begin : begin + half].astype(jnp.float32)
                + one[k, axis, 1].astype(jnp.float32)
            ).astype(jnp.bfloat16)
            two_copy(k, axis).start()

    def third_stage(k):
        to = order(k)
        for axis in range(2):
            begin = 0 if axis == 0 else half
            two_copy(k, axis).wait_recv()
            tot[k, begin : begin + half] = (
                sums[k, 0, begin : begin + half].astype(jnp.float32)
                + one[k, axis, 0].astype(jnp.float32)
                + two_in[k, axis].astype(jnp.float32)
            ).astype(jnp.bfloat16)

        @pl.when(to != level)
        def _():
            total_copy(k).start()

        @pl.when(to == level)
        def _():
            tot_in[level] = tot[k]

    def column_of(block):
        lane = lax.broadcasted_iota(jnp.int32, (rows, LANES), 1)
        return jnp.sum(jnp.where(lane == block, wcols[...], 0.0), axis=1, keepdims=True)

    tile = min(256, units)

    def iteration(k):
        from_level = order(k)

        begin = jnp.minimum(near + k, 3)
        stop = jnp.minimum(near + k + 1, 3)

        def mixes(lows, highs):
            with jax.named_scope("mix_ev"):
                each(pick(k, lows), pick(k, highs), mix_event)

        with jax.named_scope("pc_wait"):
            for relative in range(4):
                at = x.at[block_rows(from_level, 1 - core), cols(relative)]
                remote(
                    at, at, s_pc.at[0], r_pc.at[from_level * 4 + relative], pc
                ).wait_recv()

        pair = pl.ds(pl.multiple_of(from_level * 2 * rows, 2 * rows), 2 * rows)
        squares = jnp.zeros((2 * rows, LANES), jnp.float32)
        for first in range(0, features, LANES):
            value = x[pair, first : first + LANES].astype(jnp.float32)
            squares = squares + value * value
        scale = lax.rsqrt(jnp.sum(squares, axis=1, keepdims=True) / features + EPSILON)

        def hidden_tile(n):
            at = aligned(n * tile, tile)
            rows_in = x[pair, :]
            gate = scale * jnp.dot(rows_in, wg[:, at], preferred_element_type=jnp.float32)
            up = scale * jnp.dot(rows_in, wu[:, at], preferred_element_type=jnp.float32)
            hidden[:, at] = (gate / (1.0 + jnp.exp(-gate)) * up).astype(jnp.bfloat16)

        tiles = units // tile

        with jax.named_scope("hidden"):
            each(0, tiles // 2, hidden_tile)
        with jax.named_scope("third_stage"):
            @pl.when(k >= near + 2)
            def _():
                third_stage(k - 2)

        with jax.named_scope("event_a"):
            each(begin, stop, first_event)
        mixes(*METER[0])
        with jax.named_scope("hidden"):
            each(tiles // 2, tiles, hidden_tile)
        mixes(*METER[1])

        def product(core_of, relative):
            value = hidden[aligned(core_of * rows, rows), :]
            weight = wd[:, cols(relative)]
            return column_of(from_level * 2 + core_of) * jnp.dot(
                value, weight, preferred_element_type=jnp.float32
            )

        with jax.named_scope("down_out"):
            for relative in (3, 1, 2, 0):
                part_out[k, relative] = product(1 - core, relative).astype(jnp.bfloat16)
                part_copy(k, relative).start()
        with jax.named_scope("second_stage"):
            @pl.when(k >= near + 1)
            def _():
                second_stage(k - 1)

        with jax.named_scope("event_c"):
            each(begin, stop, second_event)
            each(begin, stop, third_event)
        mixes(*METER[2])
        with jax.named_scope("down_own"):
            for relative in (3, 1, 2, 0):
                value = product(core, relative)
                part_copy(k, relative).wait_recv()
                value = value + part_in[k, relative].astype(jnp.float32)

                @pl.when(k < levels - 1)
                def _():
                    sums[k, relative] = value.astype(jnp.bfloat16)

                @pl.when(k == levels - 1)
                def _():
                    @pl.when(level > 0)
                    def _():
                        fold_wait(0, relative)

                    @pl.when(level < levels - 1)
                    def _():
                        fold_wait(1, relative)

                    sums[k, relative] = (
                        value
                        + fold[0, relative].astype(jnp.float32)
                        + fold[1, relative].astype(jnp.float32)
                    ).astype(jnp.bfloat16)

                @pl.when(k < near)
                def _():
                    fold_copy(k, relative).start()

                @pl.when(k >= near)
                def _():
                    for axis in range(2):
                        if relative in (3, axis + 1):
                            one_copy(k, relative, axis).start()

        with jax.named_scope("event_d"):
            each(begin, stop, fourth_event)

    with jax.named_scope("weights_wait"):
        for copy in loads[7:]:
            copy.wait()

    each(0, levels, iteration)

    def mix_tile(q):
        for piece in range(TILE):
            mix(q * TILE + piece, 1 - piece % 2).wait_recv()
            mix(q * TILE + piece, 2).wait_recv()
        at = aligned(q * wide, wide)
        mixed[at, :] = lax.dot_general(
            y[:, at], proj[...], (((0,), (0,)), ((), ())), preferred_element_type=jnp.float32
        ).astype(jnp.bfloat16)
        pltpu.make_async_copy(mixed.at[at], mixed_out.at[at], out_sem.at[q]).start()

    each(LATE[0], LATE[1], mix_event)
    with jax.named_scope("mix_tiles"):
        each(0, tiles_of // 4, mix_tile)
    with jax.named_scope("last_third"):
        third_stage(levels - 2)
    each(LATE[1], LATE[2], mix_event)
    with jax.named_scope("mix_tiles"):
        each(tiles_of // 4, tiles_of // 2, mix_tile)
    with jax.named_scope("last_second"):
        second_stage(levels - 1)
    each(LATE[2], 2 * CHUNKS, mix_event)
    with jax.named_scope("mix_tiles"):
        each(tiles_of // 2, tiles_of, mix_tile)
    with jax.named_scope("last_third"):
        third_stage(levels - 1)
    with jax.named_scope("tot_wait"):
        for away in range(1, levels):
            source = (level + away) % levels

            @pl.when((source > level + 1) | (source < level - 1))
            def _():
                at = tot_in.at[source]
                remote(at, at, s_tot.at[0], r_tot.at[source], xn).wait_recv()
    answer = jnp.zeros((rows, part), jnp.float32)
    for source in range(levels):
        answer = answer + tot_in[source].astype(jnp.float32)
    final[...] = answer.astype(jnp.bfloat16)
    last = pltpu.make_async_copy(final, expert_out, out_sem.at[CHUNKS])
    last.start()

    with jax.named_scope("finish"):
        for relative in range(4):
            @pl.when(level < levels - 1)
            def _():
                along(level, relative, True).wait_send()

            @pl.when(level > 0)
            def _():
                along(level, relative, False).wait_send()

            partner(level, relative).wait_send()
            plane(level, relative, 0).wait_send()

        @pl.when(has_next)
        def _():
            rim_copy.wait_send()

        for away in range(1, levels):
            table_to(away).wait_send()
        for level_of in range(levels):
            table_pc(level_of).wait_send()

        def finish(k):
            from_level = order(k)
            up = from_level < level
            relay = jnp.where(up, level < levels - 1, level > 0)
            for relative in range(4):
                @pl.when((k < levels - 1) & relay)
                def _():
                    along(from_level, relative, up).wait_send()

                @pl.when(k < levels - 1)
                def _():
                    plane(from_level, relative, early_rows).wait_send()
                    partner(from_level, relative).wait_send()

                part_copy(k, relative).wait_send()

                @pl.when(k < near)
                def _():
                    fold_copy(k, relative).wait_send()

            @pl.when(k >= near)
            def _():
                for axis in range(2):
                    one_copy(k, axis + 1, axis).wait_send()
                    one_copy(k, 3, axis).wait_send()
                    two_copy(k, axis).wait_send()

            @pl.when((from_level != level) & (k >= near))
            def _():
                total_copy(k).wait_send()

        each(0, levels, finish)

        def finish_mix(q):
            for way in range(3):
                mix(q, way).wait_send()

        def finish_out(q):
            at = aligned(q * wide, wide)
            pltpu.make_async_copy(mixed.at[at], mixed_out.at[at], out_sem.at[q]).wait()

        each(0, CHUNKS, finish_mix)
        each(0, tiles_of, finish_out)
        last.wait()


def copy_kernel(mixed, expert, mixed_out, expert_out, held, held_expert, in_sem, out_sem):
    size = mixed.shape[0] // COPIES
    pairs = []
    for i in range(COPIES):
        at = pl.ds(i * size, size)
        pairs.append((mixed.at[at], held.at[at], mixed_out.at[at]))
    pairs.append((expert, held_expert, expert_out))
    reads = [
        pltpu.make_async_copy(src, mid, in_sem.at[i]) for i, (src, mid, _) in enumerate(pairs)
    ]
    writes = [
        pltpu.make_async_copy(mid, dst, out_sem.at[i]) for i, (_, mid, dst) in enumerate(pairs)
    ]
    for read in reads:
        read.start()
    for read, write in zip(reads, writes):
        read.wait()
        write.start()
    for write in writes:
        write.wait()


def copied(mixed, expert):
    anywhere = pl.BlockSpec(memory_space=pl.ANY)
    return pl.pallas_call(
        copy_kernel,
        out_shape=tuple(jax.ShapeDtypeStruct(v.shape, v.dtype) for v in (mixed, expert)),
        in_specs=[anywhere] * 2,
        out_specs=(anywhere, anywhere),
        scratch_shapes=[
            pltpu.VMEM(mixed.shape, mixed.dtype), pltpu.VMEM(expert.shape, expert.dtype),
            pltpu.SemaphoreType.DMA((COPIES + 1,)), pltpu.SemaphoreType.DMA((COPIES + 1,)),
        ],
    )(mixed, expert)


def fused(*args):
    (conv_input, out_gate, in_gate, conv_taps, mixer_proj, token_rows, routes, route_weights,
     expert_gate, expert_up, expert_down) = args
    tp, experts = lax.axis_size("tp"), lax.axis_size("ep")
    rows, part = token_rows.shape
    features = part * tp
    units = expert_gate.shape[2]
    width, length = conv_input.shape
    levels, half = experts // 2, rows // 2
    early_rows = rows * EARLY_PART[0] // EARLY_PART[1] // 16 * 16
    bf16, f32 = jnp.bfloat16, jnp.float32
    dma = pltpu.SemaphoreType.DMA
    hold = pltpu.VMEM
    scratch = [
        hold((experts * rows, features), bf16),
        hold((features, units), bf16), hold((features, units), bf16), hold((units, features), bf16),
        hold((width, length), bf16), hold((width, length), bf16), hold((width, length), bf16),
        hold((width, length + LANES), bf16),
        hold((tp * width, length), bf16),
        hold(mixer_proj.shape, bf16),
        hold((LANES, max(width, rows)), f32),
        hold(conv_taps.shape, f32),
        hold((2, rows), jnp.int32), hold((2, rows), f32),
        hold((experts, experts, rows), f32),
        hold((rows, LANES), f32),
        hold((2 * rows, units), bf16),
        hold((levels, 4, rows, part), bf16), hold((levels, 4, rows, part), bf16),
        hold((levels, 4, rows, part), bf16),
        hold((2, 4, rows, part), bf16),
        hold((levels, 2, 2, half, part), bf16),
        hold((levels, 2, half, part), bf16), hold((levels, 2, half, part), bf16),
        hold((levels, rows, part), bf16), hold((levels, rows, part), bf16),
        hold((length, part), bf16),
        hold((rows, part), bf16),
        dma((11,)),
        dma((levels * 4,)), dma((levels * 4,)),
        dma((levels * 8,)), dma((levels * 4,)),
        dma((levels * 4,)), dma((levels * 4,)),
        dma((levels * 2,)), dma((experts,)),
        dma, dma,
        dma((CHUNKS * 3,)), dma((CHUNKS * 3,)),
        dma((levels * 4,)), dma((levels * 4,)),
        dma((8,)), dma((8,)),
        dma((levels * 4,)), dma((levels * 4,)),
        dma((levels * 2,)), dma((levels * 2,)),
        dma((levels,)), dma((levels,)),
        dma((CHUNKS + 1,)),
    ]
    anywhere = pl.BlockSpec(memory_space=pl.ANY)
    return pl.pallas_call(
        functools.partial(fused_kernel, early_rows),
        out_shape=(
            jax.ShapeDtypeStruct((length, part), bf16), jax.ShapeDtypeStruct((rows, part), bf16)
        ),
        in_specs=[anywhere] * 11,
        out_specs=(anywhere, anywhere),
        scratch_shapes=scratch,
        compiler_params=pltpu.CompilerParams(
            collective_id=0, has_side_effects=True, vmem_limit_bytes=67043328
        ),
    )(
        conv_input, out_gate, in_gate, conv_taps, mixer_proj, token_rows, routes.T,
        route_weights.T, expert_gate[0], expert_up[0], expert_down[0],
    )


def passed_along(value, axis, by):
    devices = lax.axis_size(axis)
    pairs = [(i, i + by) for i in range(devices) if 0 <= i + by < devices]
    return lax.ppermute(value, axis, pairs)


def rotated(value, by):
    devices = lax.axis_size("ep")
    return lax.ppermute(value, "ep", [(i, (i + by) % devices) for i in range(devices)])


def routing(route_ids, capacity, experts):
    rows = route_ids.shape[0]
    names = jnp.arange(experts, dtype=jnp.int32)[None, :]
    hits = [(route_ids[:, k][:, None] == names) for k in range(2)]
    both = (hits[0] | hits[1]).astype(jnp.bfloat16)
    index = jnp.arange(rows, dtype=jnp.int32)
    lower = (index[:, None] > index[None, :]).astype(jnp.bfloat16)
    earlier = jnp.dot(lower, both, preferred_element_type=jnp.float32)
    away = lax.rem(route_ids - lax.axis_index("ep") + experts, experts)
    places = []
    for k in range(2):
        rank = jnp.sum(jnp.where(hits[k], earlier, 0.0), axis=1).astype(jnp.int32)
        places.append(away[:, k] * capacity + rank)
    return places


def expert_hidden(part_in, row_scale, gate_weight, up_weight):
    gate_sum = jnp.dot(part_in, gate_weight, preferred_element_type=jnp.float32)
    up_sum = jnp.dot(part_in, up_weight, preferred_element_type=jnp.float32)
    return (jax.nn.silu(row_scale * gate_sum) * (row_scale * up_sum)).astype(jnp.bfloat16)


def product(hidden, down):
    return jnp.dot(hidden, down, preferred_element_type=jnp.float32).astype(jnp.bfloat16)


def general(
    conv_input,
    out_gate,
    in_gate,
    conv_taps,
    mixer_proj,
    token_rows,
    routes,
    route_weights,
    expert_gate,
    expert_up,
    expert_down,
):
    tp = lax.axis_size("tp")
    here = lax.axis_index("tp")
    width_part = conv_input.shape[0]
    length = conv_input.shape[1]
    local_taps = lax.dynamic_slice_in_dim(conv_taps, here * width_part, width_part, 1)

    experts = lax.axis_size("ep")
    rows_b, cols_part = token_rows.shape
    capacity = 4 * rows_b // experts
    slot_total = experts * capacity
    feature_count = cols_part * tp
    places = routing(routes, capacity, experts)
    slots = jnp.arange(slot_total, dtype=jnp.int32)
    picks = [(slots[:, None] == places[k][None, :]) for k in range(2)]
    chosen = (picks[0] | picks[1]).astype(jnp.bfloat16)
    buffer = jnp.dot(chosen, token_rows, preferred_element_type=jnp.float32).astype(jnp.bfloat16)

    z_rows = (conv_input.astype(jnp.float32) * in_gate.astype(jnp.float32)).astype(jnp.bfloat16)
    rim_rows = passed_along(z_rows[:, length - (KERNEL - 1) :], "ep", 1)
    longer = jnp.concatenate([rim_rows, z_rows], axis=1).astype(jnp.float32)
    conv_sum = jnp.zeros(z_rows.shape, jnp.float32)
    for lag_index in range(KERNEL):
        begin = KERNEL - 1 - lag_index
        conv_sum = conv_sum + local_taps[lag_index][:, None] * longer[:, begin : begin + length]
    gated = (out_gate.astype(jnp.float32) * conv_sum).astype(jnp.bfloat16)

    gated, buffer = lax.optimization_barrier((gated, buffer))
    arrived = [
        rotated(buffer[d * capacity : (d + 1) * capacity], d) if d else buffer[:capacity]
        for d in range(experts)
    ]
    chunk_parts = experts // PIECES
    chunks = [
        jnp.concatenate(arrived[c * chunk_parts : (c + 1) * chunk_parts], axis=0)
        for c in range(PIECES)
    ]
    gate_weight, up_weight, down_weight = expert_gate[0], expert_up[0], expert_down[0]

    def squares_of(part_in):
        return jnp.sum(jnp.square(part_in.astype(jnp.float32)), axis=1)

    def scale_of(squares):
        return lax.rsqrt(squares / feature_count + EPSILON)[:, None]

    outs, returned = [], []

    def send_back(c):
        for i in range(chunk_parts):
            d = c * chunk_parts + i
            block = outs[c][i * capacity : (i + 1) * capacity]
            returned.append(rotated(block, -d) if d else block)

    proj = mixer_proj
    mixer_in = lax.all_gather(gated, "tp", axis=0, tiled=True)
    for c, own in enumerate(chunks):
        part_in = lax.all_gather(own, "tp", axis=1, tiled=True)
        hidden = expert_hidden(part_in, scale_of(squares_of(part_in)), gate_weight, up_weight)
        outs.append(
            lax.psum_scatter(
                product(hidden, down_weight), "tp", scatter_dimension=1, tiled=True
            )
        )
        send_back(c)

    returned = jnp.concatenate(returned, axis=0)
    weights = sum(
        jnp.where(slots[None, :] == places[k][:, None], route_weights[:, k][:, None], 0.0)
        for k in range(2)
    )
    high = weights.astype(jnp.bfloat16)
    low = (weights - high.astype(jnp.float32)).astype(jnp.bfloat16)
    both = jnp.dot(
        jnp.concatenate([high, low], axis=0), returned, preferred_element_type=jnp.float32
    )
    expert_out = (both[:rows_b] + both[rows_b:]).astype(jnp.bfloat16)

    mixed_out = lax.dot_general(
        mixer_in, proj, (((0,), (0,)), ((), ())), preferred_element_type=jnp.float32
    ).astype(jnp.bfloat16)
    return (mixed_out, expert_out)


def body(*args):
    square = lax.axis_size("tp") == 4 and lax.axis_size("ep") == 8
    return copied(*fused(*args)) if square else general(*args)


def solution(mesh):
    return jax.shard_map(
        body,
        mesh=mesh,
        in_specs=(
            P("tp", "ep"),
            P("tp", "ep"),
            P("tp", "ep"),
            P(),
            P(None, "tp"),
            P("ep", "tp"),
            P("ep", None),
            P("ep", None),
            P("ep", None, "tp"),
            P("ep", None, "tp"),
            P("ep", "tp", None),
        ),
        out_specs=(P("ep", "tp"), P("ep", "tp")),
        check_vma=False,
    )
```
